128 devices in a mesh: sp: 64 (over z, y, x), tp: 2 (over core).
Axes of the slice: x: 4, y: 4, z: 4, core: 2. Of those that a mesh axis runs over, the one named last changes fastest.
Arguments:
- wide_inputs: bfloat16 [8192, 512], P('sp', 'tp'), may hold values from -6 to 6
- narrow_inputs: bfloat16 [8192, 512], P('sp', 'tp'), may hold values from -6 to 6
- wide_poles: float32 [2, 2, 32, 64], P(None, None, 'tp'), may hold values from -3.1416 to 3.1416, as said below
- narrow_poles: float32 [2, 2, 32, 32], P(None, None, 'tp'), may hold values from -3.1416 to 3.1416, as said below
- step_sizes: float32 [2, 2, 32], P(None, None, 'tp'), may hold values from 0 to 1, as said below
- forget: float32 [2, 2, 32, 8192], P(None, None, 'tp', 'sp'), may hold values from 0 to 2.2
- wide_in_map: float32 [2, 2, 32, 16, 64], P(None, None, 'tp'), may hold values from -2.5 to 2.5
- narrow_in_map: float32 [2, 2, 32, 16, 32], P(None, None, 'tp'), may hold values from -2.5 to 2.5
- wide_out_map: float32 [2, 2, 32, 16, 64], P(None, None, 'tp'), may hold values from -1.25 to 1.25
- narrow_out_map: float32 [2, 2, 32, 16, 32], P(None, None, 'tp'), may hold values from -2 to 2
- skip_weight: bfloat16 [2, 512], P(None, 'tp'), may hold values from -6 to 6
- gate_mix: bfloat16 [2, 32, 16, 16], P(None, 'tp'), may hold values from -1.5 to 1.5
- residual: bfloat16 [8192, 2048], P(('sp', 'tp')), may hold values from -6 to 6
- mixer_gain: float32 [1024], replicated, may hold values from 0.1 to 1.9
- out_proj: bfloat16 [1024, 2048], replicated, may hold values from -0.1875 to 0.1875
- ffn_gain: float32 [2048], replicated, may hold values from 0.1 to 1.9
- routes: int32 [8192, 2], P(('sp', 'tp')), may hold values from 0 to 127, all different within a row; in each aligned block of 64 rows (0 to 63, 64 to 127, ...) at most 2 rows name the same one
- route_weights: float32 [8192, 2], P(('sp', 'tp')), may hold values from 0.1 to 1
- gate_proj: bfloat16 [128, 2048, 1408], P(('sp', 'tp')), may hold values from -0.125 to 0.125
- up_proj: bfloat16 [128, 2048, 1408], P(('sp', 'tp')), may hold values from -0.125 to 0.125
- down_proj: bfloat16 [128, 1408, 2048], P(('sp', 'tp')), may hold values from -0.15625 to 0.15625
Outputs:
- layer_out: bfloat16 [8192, 2048], P(('sp', 'tp'))
The draws below stay inside these ranges and needn't reach their ends.
Inputs may be any that keep to these rules, and one draw needn't show every extreme that they name: `routes`: in each aligned block of 64 rows (the rows of one device), no expert is named by more than 2 entries, and the 2 experts of a row differ. `wide_poles`: along dimension 1, entry 0 (the real part) is negative and entry 1 (the imaginary part) is at least 0.1 in magnitude. `narrow_poles`: along dimension 1, entry 0 (the real part) is negative and entry 1 (the imaginary part) is at least 0.1 in magnitude. `step_sizes`: Positive.
All inputs are finite; a program needn't handle non-finite values.
Results may differ from the reference program's by a relative error of at most 0.014.
Values may be sent and summed in bfloat16 or wider, within the bound.
A program may use at most 192 MiB of HBM per device.

```python
import math
import jax
import jax.numpy as jnp
import numpy as np
from jax import lax

D = 2048
GROUPS = 32
CHANNELS = 16
WIDE_STATE = 64
NARROW_STATE = 32
FE = 1408
TOP = 2
TOK_DEV = 128
TOKENS = 8192
ROWS = 64
SETW = 512
EXPERTS = 128
CAP = 2


def pick_slow(key):
    chance = 0.5
    return jax.random.bernoulli(jax.random.fold_in(key, 101), chance, (2, 2, GROUPS))


def make_poles(key, which, states):
    slow = pick_slow(key)[:, which]
    keys = jax.random.split(jax.random.fold_in(key, 11 + which), 4)
    slow_rate = jnp.exp(jax.random.uniform(keys[0], (2, GROUPS, states), jnp.float32, math.log(0.05), math.log(0.5))) / TOKENS
    fast_rate = jnp.exp(jax.random.uniform(keys[1], (2, GROUPS, states), jnp.float32, math.log(0.02), math.log(0.1)))
    decay_re = -jnp.where(slow[:, :, None], slow_rate, fast_rate)
    signs = jnp.where(jax.random.bernoulli(keys[3], 0.5, (2, GROUPS, states)), 1.0, -1.0)
    decay_im = jax.random.uniform(keys[2], (2, GROUPS, states), jnp.float32, 0.1, 3.14) * signs
    return jnp.stack([decay_re, decay_im], axis=1).astype(jnp.float32)


def draw_wide_poles(key, part):
    return make_poles(key, 0, WIDE_STATE)


def draw_narrow_poles(key, part):
    return make_poles(key, 1, NARROW_STATE)


def draw_step_sizes(key, part):
    slow = pick_slow(key)
    base = jnp.exp(jax.random.uniform(jax.random.fold_in(key, 21), (2, 2, GROUPS), jnp.float32, math.log(0.5), math.log(2.0)))
    return (base * jnp.where(slow, math.sqrt(0.4 / TOKENS), 0.3)).astype(jnp.float32)


def draw_forget(key, part):
    keys = jax.random.split(jax.random.fold_in(key, 31), 3)
    blocks = TOKENS // TOK_DEV
    factor = jnp.exp(jax.random.uniform(keys[0], (2, 2, GROUPS, blocks), jnp.float32, math.log(0.1), math.log(1.0)))
    decay_speed = jnp.repeat(factor, TOK_DEV, axis=3) / TOKENS
    spots = jax.random.randint(keys[1], (2, 2, GROUPS, 3), 0, TOKENS)
    total_quantity = jax.random.uniform(keys[2], (2, 2, GROUPS, 3), jnp.float32, 0.22, 0.69)
    slot_positions = jnp.arange(TOKENS)[None, None, None, None, :] == spots[:, :, :, :, None]
    signal_segments = jnp.sum(jnp.where(slot_positions, total_quantity[:, :, :, :, None], 0.0), axis=3)
    return (decay_speed + signal_segments).astype(jnp.float32)


def block_levels(stream_key, extent, cuts, least, top_value):
    factor_of = 1.0
    for position, parts in cuts:
        heights = jax.random.uniform(jax.random.fold_in(jax.random.fold_in(stream_key, 6), position), (parts,), jnp.float32, least / len(cuts), top_value / len(cuts))
        factor_of = factor_of * jnp.repeat(jnp.exp(heights), extent[position] // parts).reshape((-1,) + (1,) * (len(extent) - 1 - position))
    return factor_of


def assign_block(stream_key, own, number, rows, number_of, top, reach, skew):
    sequence = jax.random.permutation(stream_key, number_of)
    packed, common = shares(number_of, rows * top, reach, skew, True), shares(number_of, rows * top, reach, skew, False)
    places = jnp.arange(number_of)

    def named(tallies, rotation):
        used = int((tallies > 0).sum())
        fixed = max(1, used // 4)
        shifted = fixed + (places - fixed + rotation * (used - fixed)) % max(1, number_of - fixed)
        return jnp.zeros((number_of,), jnp.int32).at[sequence[jnp.where(places < fixed, places, shifted)]].set(jnp.asarray(tallies, jnp.int32))

    tallies = jnp.where(number % 4 == 0, named(packed, number // 4), named(common, number - number // 4 - 1))
    mixed = jax.random.permutation(jax.random.fold_in(own, 3), number_of)
    donor, sink = mixed[0:number_of // 2 * 2:2], mixed[1:number_of // 2 * 2:2]
    slack = jnp.minimum(tallies[donor] - 1, reach - tallies[sink]) // 2
    slack = jnp.where((donor == sequence[0]) | (sink == sequence[0]) | (tallies[sink] == 0), 0, jnp.maximum(slack, 0))
    shifted = jax.random.randint(jax.random.fold_in(own, 4), (number_of // 2,), 0, 1 << 20) % (slack + 1)
    tallies = tallies.at[donor].add(-shifted).at[sink].add(shifted)
    labels = jnp.searchsorted(jnp.cumsum(tallies), jnp.arange(rows * top), side="right").astype(jnp.int32)
    table = labels.reshape(top, rows).T
    table = table[jax.random.permutation(jax.random.fold_in(own, 1), rows)]
    rotation = jax.random.randint(jax.random.fold_in(own, 2), (rows, 1), 0, top)
    return jnp.take_along_axis(table, (jnp.arange(top)[None, :] + rotation) % top, axis=1)


def shares(count, total, bound, lean, full):
    weights = [(1 << 20) // math.isqrt(rank ** lean) + 1 for rank in range(1, count + 1)]
    largest = bound if full else min(bound, max(-(-total // count), total * weights[0] // sum(weights)))
    least = 1 if total - largest >= count - 1 else 0
    counts, spare = [largest] + [least] * (count - 1), total - largest - least * (count - 1)
    while spare > 0:
        candidates = [i for i in range(1, count) if counts[i] < largest] or [i for i in range(1, count) if counts[i] < bound]
        pool, left = sum([weights[i] for i in candidates]), spare
        for i in candidates:
            more = min(bound - counts[i], max(1, left * weights[i] // pool), spare)
            counts[i] = counts[i] + more
            spare = spare - more
    return np.array(counts)


def normal_values(key, shape, spread, reach, cuts=(), kind=jnp.bfloat16):
    values = spread * jax.random.normal(key, shape, jnp.float32)
    if cuts:
        values = values * block_levels(key, shape, cuts, -0.22, 0.18)
    return jnp.clip(values, -reach, reach).astype(kind)


def setup_inputs(seed: int = 0) -> dict:
    key_list = jax.random.split(jax.random.key(seed), 22)
    wide_inputs = normal_values(key_list[0], (TOKENS, SETW), 1.0, 6.0, ((0, 64), (1, 2)))
    narrow_inputs = normal_values(key_list[1], (TOKENS, SETW), 1.0, 6.0, ((0, 64), (1, 2)))
    wide_poles = draw_wide_poles(jax.random.fold_in(key_list[21], 71), 0)
    narrow_poles = draw_narrow_poles(jax.random.fold_in(key_list[21], 71), 0)
    step_sizes = draw_step_sizes(jax.random.fold_in(key_list[21], 71), 0)
    forget = draw_forget(jax.random.fold_in(key_list[21], 71), 0)
    wide_in_map = normal_values(key_list[6], (2, 2, GROUPS, CHANNELS, WIDE_STATE), ((2 * CHANNELS) ** -0.5), 2.5, ((2, 2),), jnp.float32)
    narrow_in_map = normal_values(key_list[7], (2, 2, GROUPS, CHANNELS, NARROW_STATE), ((2 * CHANNELS) ** -0.5), 2.5, ((2, 2),), jnp.float32)
    wide_out_map = normal_values(key_list[8], (2, 2, GROUPS, CHANNELS, WIDE_STATE), ((2 * WIDE_STATE) ** -0.5), 1.25, ((2, 2),), jnp.float32)
    narrow_out_map = normal_values(key_list[9], (2, 2, GROUPS, CHANNELS, NARROW_STATE), ((2 * NARROW_STATE) ** -0.5), 2.0, ((2, 2),), jnp.float32)
    skip_weight = normal_values(key_list[10], (2, SETW), 1.0, 6.0, ((1, 2),))
    gate_mix = normal_values(key_list[11], (2, GROUPS, CHANNELS, CHANNELS), CHANNELS ** -0.5, 1.5, ((1, 2),))
    residual = normal_values(key_list[12], (TOKENS, D), 1.0, 6.0, ((0, 128),))
    mixer_gain = jnp.clip(1.0 + 0.18 * jax.random.normal(key_list[13], (2 * SETW,), jnp.float32), 0.1, 1.9)
    out_proj = normal_values(key_list[14], (2 * SETW, D), (2 * SETW) ** -0.5, 0.1875)
    ffn_gain = jnp.clip(1.0 + 0.18 * jax.random.normal(key_list[15], (D,), jnp.float32), 0.1, 1.9)
    routes_keys = jax.random.split(jax.random.fold_in(key_list[16], 1), TOKENS // ROWS)
    routes_turns = jax.random.permutation(jax.random.fold_in(key_list[16], 3), TOKENS // ROWS)
    routes = jax.vmap(lambda own, number: assign_block(jax.random.fold_in(key_list[16], 2), own, number, ROWS, EXPERTS, TOP, CAP, 2))(routes_keys, routes_turns).reshape((TOKENS, TOP))
    route_weights = jnp.clip(jnp.exp(math.log(1.0) - 2.3025851 * jax.random.uniform(key_list[17], (TOKENS, TOP), jnp.float32) ** block_levels(key_list[17], (TOKENS, TOP), ((0, 128),), -0.2, 0.2)), 0.1, 1.0)
    gate_proj = normal_values(key_list[18], (EXPERTS, D, FE), D ** -0.5, 0.125, ((0, 128),))
    up_proj = normal_values(key_list[19], (EXPERTS, D, FE), D ** -0.5, 0.125, ((0, 128),))
    down_proj = normal_values(key_list[20], (EXPERTS, FE, D), FE ** -0.5, 0.15625, ((0, 128),))
    return dict(wide_inputs=wide_inputs, narrow_inputs=narrow_inputs, wide_poles=wide_poles, narrow_poles=narrow_poles, step_sizes=step_sizes, forget=forget, wide_in_map=wide_in_map, narrow_in_map=narrow_in_map, wide_out_map=wide_out_map, narrow_out_map=narrow_out_map, skip_weight=skip_weight, gate_mix=gate_mix, residual=residual, mixer_gain=mixer_gain, out_proj=out_proj, ffn_gain=ffn_gain, routes=routes, route_weights=route_weights, gate_proj=gate_proj, up_proj=up_proj, down_proj=down_proj)


maximum_value = lax.Precision.HIGHEST
epsilon = 1e-06

def pair_step(first, second):
    first_ar, first_ai, first_br, first_bi = first
    second_ar, second_ai, second_br, second_bi = second
    return (second_ar * first_ar - second_ai * first_ai, second_ar * first_ai + second_ai * first_ar, second_ar * first_br - second_ai * first_bi + second_br, second_ar * first_bi + second_ai * first_br + second_bi)

def block_diagonal_in(matrix):
    groups, channels, states = matrix.shape
    identity = jnp.eye(groups, dtype=jnp.float32)
    return jnp.einsum('gcs,gh->gchs', matrix, identity).reshape(groups * channels, groups * states)

def block_diagonal_out(matrix):
    groups, channels, states = matrix.shape
    identity = jnp.eye(groups, dtype=jnp.float32)
    return jnp.einsum('gcs,gh->gshc', matrix, identity).reshape(groups * states, groups * channels)

def local_states(input_sequence, poles, step, decay, in_map, backward):
    decay_re = poles[0]
    decay_im = poles[1]
    states = decay_re.shape[1]
    growth = jnp.exp(decay_re)
    numer_re = growth * jnp.cos(decay_im) - 1.0
    numer_im = growth * jnp.sin(decay_im)
    denom = decay_re * decay_re + decay_im * decay_im
    factor_re = (numer_re * decay_re + numer_im * decay_im) / denom * step[:, None]
    factor_im = (numer_im * decay_re - numer_re * decay_im) / denom * step[:, None]
    input_real = factor_re[:, None, :] * in_map[0] - factor_im[:, None, :] * in_map[1]
    input_imaginary = factor_re[:, None, :] * in_map[1] + factor_im[:, None, :] * in_map[0]
    driven_real = jnp.dot(input_sequence, block_diagonal_in(input_real), precision=maximum_value)
    driven_imaginary = jnp.dot(input_sequence, block_diagonal_in(input_imaginary), precision=maximum_value)
    flat_re = decay_re.reshape(-1)[None]
    flat_im = decay_im.reshape(-1)[None]
    magnitude = jnp.exp(flat_re - jnp.repeat(jnp.transpose(decay), states, axis=1))
    return lax.associative_scan(pair_step, (magnitude * jnp.cos(flat_im), magnitude * jnp.sin(flat_im), driven_real, driven_imaginary), reverse=backward, axis=0)

def read_out(hidden_state_real, hidden_state_imaginary, output_matrix):
    return jnp.dot(hidden_state_real, block_diagonal_out(output_matrix[0]), precision=maximum_value) - jnp.dot(hidden_state_imaginary, block_diagonal_out(output_matrix[1]), precision=maximum_value)

def finish_set(input_sequence, total, skip_row, gate_block):
    shaped = total + skip_row.astype(jnp.float32)[None] * input_sequence
    active = jax.nn.gelu(shaped, approximate=True)
    gate_full = block_diagonal_in(gate_block.astype(jnp.float32))
    opened = jax.nn.sigmoid(jnp.dot(active, gate_full, precision=maximum_value))
    return (active * opened).astype(jnp.bfloat16)

def run_set(inputs, poles, steps, decay, in_map, output_matrix, skip_row, gate_block):
    blocks = TOKENS // TOK_DEV
    groups = poles.shape[2]
    states = poles.shape[3]
    input_sequence = inputs.astype(jnp.float32)
    signal_blocks = input_sequence.reshape(blocks, TOK_DEV, groups * CHANNELS)
    total = jnp.zeros((TOKENS, groups * CHANNELS), jnp.float32)
    for direction in range(2):
        decay_blocks = jnp.transpose(decay[direction].reshape(groups, blocks, TOK_DEV), (1, 0, 2))
        backward = direction == 1
        edge = 0 if backward else -1

        def stepper(carry, pieces):
            piece, piece_decay = pieces
            prod_re, prod_im, hidden_state_real, hidden_state_imaginary = local_states(piece, poles[direction], steps[direction], piece_decay, in_map[direction], backward)
            full_re = hidden_state_real + prod_re * carry[0][None] - prod_im * carry[1][None]
            full_im = hidden_state_imaginary + prod_re * carry[1][None] + prod_im * carry[0][None]
            return ((full_re[edge], full_im[edge]), read_out(full_re, full_im, output_matrix[direction]))
        start = (jnp.zeros((groups * states,), jnp.float32), jnp.zeros((groups * states,), jnp.float32))
        _, outputs = lax.scan(stepper, start, (signal_blocks, decay_blocks), reverse=backward)
        total = total + outputs.reshape(TOKENS, groups * CHANNELS)
    return finish_set(input_sequence, total, skip_row, gate_block)

def reference(wide_inputs, narrow_inputs, wide_poles, narrow_poles, step_sizes, forget, wide_in_map, narrow_in_map, wide_out_map, narrow_out_map, skip_weight, gate_mix, residual, mixer_gain, out_proj, ffn_gain, routes, route_weights, gate_proj, up_proj, down_proj):
    wide_mix = run_set(wide_inputs, wide_poles, step_sizes[:, 0], forget[:, 0], wide_in_map, wide_out_map, skip_weight[0], gate_mix[0])
    narrow_mix = run_set(narrow_inputs, narrow_poles, step_sizes[:, 1], forget[:, 1], narrow_in_map, narrow_out_map, skip_weight[1], gate_mix[1])
    joined = jnp.concatenate([wide_mix, narrow_mix], axis=1).astype(jnp.float32)
    scale = lax.rsqrt(lax.optimization_barrier(jnp.mean(joined * joined, axis=1, keepdims=True)) + epsilon)
    mixed = (joined * scale * mixer_gain).astype(jnp.bfloat16)
    projected = jnp.dot(mixed, out_proj, preferred_element_type=jnp.float32)
    hidden1 = (residual.astype(jnp.float32) + projected).astype(jnp.bfloat16)
    hidden_wide = hidden1.astype(jnp.float32)
    normed = (hidden_wide * lax.rsqrt(lax.optimization_barrier(jnp.mean(hidden_wide * hidden_wide, axis=1, keepdims=True)) + epsilon) * ffn_gain).astype(jnp.bfloat16)
    share = route_weights / lax.optimization_barrier(jnp.sum(route_weights, axis=1, keepdims=True))
    blocks = TOKENS // ROWS
    picks = routes.reshape(blocks, ROWS * TOP)
    onehot = (picks[:, :, None] == jnp.arange(EXPERTS, dtype=jnp.int32)[None, None, :]).astype(jnp.int32)
    rank = lax.optimization_barrier(jnp.sum((jnp.cumsum(onehot, axis=1) - onehot) * onehot, axis=2))
    anchor = (jnp.arange(blocks, dtype=jnp.int32) * CAP)[:, None]
    place = (picks * (blocks * CAP) + anchor + rank).reshape(-1).astype(jnp.int32)
    sectioning = jnp.zeros((EXPERTS * blocks * CAP, D), jnp.bfloat16).at[place].set(jnp.repeat(normed, TOP, axis=0))

    def apply_expert(pieces):
        rows_in, gate_w, up_w, down_w = pieces
        gate_val = jnp.dot(rows_in, gate_w, preferred_element_type=jnp.float32)
        up_val = jnp.dot(rows_in, up_w, preferred_element_type=jnp.float32)
        expert_hidden = (jax.nn.silu(gate_val) * up_val).astype(jnp.bfloat16)
        return jnp.dot(expert_hidden, down_w, preferred_element_type=jnp.float32).astype(jnp.bfloat16)
    served = lax.map(apply_expert, (sectioning.reshape(EXPERTS, blocks * CAP, D), gate_proj, up_proj, down_proj))
    taken = jnp.take(served.reshape(-1, D), place, axis=0).reshape(TOKENS, TOP, D).astype(jnp.float32)
    result = hidden1.astype(jnp.float32) + lax.optimization_barrier(jnp.sum(share[:, :, None] * taken, axis=1))
    return result.astype(jnp.bfloat16)
```

```python
import functools

import jax
import jax.numpy as jnp
from jax import lax
from jax.experimental import pallas as pl
from jax.experimental.pallas import tpu as pltpu
from jax.sharding import Mesh
from jax.sharding import PartitionSpec as P

SP = ("sp_0", "sp_1", "sp_2")
SP_TP = ("sp_0", "sp_1", "sp_2", "tp")
MESH = pl.DeviceIdType.MESH
epsilon = 1e-06
F32 = jnp.float32
BF16 = jnp.bfloat16
NL = 1536
SETS = ((64, 0), (32, 1024))
CHUNK = 512


def dot(a, b):
    return lax.dot_general(a, b, (((1,), (0,)), ((), ())), preferred_element_type=F32)


def dot_nt(a, b):
    return lax.dot_general(a, b, (((1,), (1,)), ((), ())), preferred_element_type=F32)


def split3(x):
    first = x.astype(BF16)
    rest = x - first.astype(F32)
    second = rest.astype(BF16)
    third = (rest - second.astype(F32)).astype(BF16)
    return first, second, third


def iota(shape, dim):
    return lax.broadcasted_iota(jnp.int32, shape, dim)


def cmul(ar, ai, br, bi):
    return ar * br - ai * bi, ar * bi + ai * br


def square(ar, ai):
    return ar * ar - ai * ai, 2.0 * ar * ai


def mixer_kernel(
    uw_ref, un_ref, pw_ref, pn_ref, step_ref, forget_ref, inw_ref, inn_ref, ow_ref, on_ref,
    skip_ref, gate_ref,
    out_ref,
    win_w, win_n, wout_w, wout_n, xs, es, spread, carry_ref, prod_ref, lam_ref, send, recv, mine,
    send_sem, recv_sem, tp_send, tp_recv,
):
    axes = ("sp_2", "sp_1", "sp_0")
    pos = [lax.axis_index(a) for a in axes]
    core = lax.axis_index("tp")

    barrier = pltpu.get_barrier_semaphore()
    for a, p in zip(axes, pos):
        for o in (1, 2, 3):
            pl.semaphore_signal(barrier, inc=1, device_id={a: lax.rem(p + o, 4)}, device_id_type=MESH)
    pl.semaphore_signal(barrier, inc=1, device_id={"tp": 1 - core}, device_id_type=MESH)

    for s, (p_ref, in_ref, o_ref, win, wout) in enumerate(
        ((pw_ref, inw_ref, ow_ref, win_w, wout_w), (pn_ref, inn_ref, on_ref, win_n, wout_n))
    ):
        n, first = SETS[s]
        tile_r = iota((n, 8 * n), 0)
        tile_c = iota((n, 8 * n), 1)
        tiler = (tile_r == lax.rem(tile_c, n)).astype(BF16)
        wr = iota((128, 8 * n), 0)
        wc = iota((128, 8 * n), 1)
        keep = (wr // 16) == (wc // n)
        for d in range(2):
            pr = p_ref[d, 0]
            pi = p_ref[d, 1]
            grow = jnp.exp(pr)
            lre = grow * jnp.cos(pi)
            lim = grow * jnp.sin(pi)
            nre = lre - 1.0
            scale = step_ref[d, s] / (pr * pr + pi * pi)
            fre = (nre * pr + lim * pi) * scale
            fim = (lim * pr - nre * pi) * scale
            for ri, lam in ((0, lre), (1, lim)):
                parts = jnp.concatenate(split3(lam), axis=0)
                for h in range(2):
                    wide = dot(parts, tiler)
                    gr = lax.rem(iota((48, 8 * n), 0), 16)
                    gc = iota((48, 8 * n), 1) // n + 8 * h
                    row = jnp.sum(jnp.where(gr == gc, wide, 0.0), axis=0, keepdims=True)
                    lam_ref[2 * d + ri : 2 * d + ri + 1, first + 8 * n * h : first + 8 * n * (h + 1)] = row
            ere, eim = [], []
            for g in range(16):
                a = in_ref[d, 0, g * 16 : (g + 1) * 16, :]
                b = in_ref[d, 1, g * 16 : (g + 1) * 16, :]
                fr, fi = fre[g : g + 1], fim[g : g + 1]
                ere.append((fr * a - fi * b).astype(BF16))
                eim.append((fr * b + fi * a).astype(BF16))
            for h in range(2):
                for ri, rows in ((0, ere), (1, eim)):
                    part = jnp.concatenate(rows[8 * h : 8 * h + 8], axis=0)
                    win[d, ri, h] = jnp.where(keep, dot(part, tiler), 0.0).astype(BF16)
                    o = o_ref[d, ri, h * 128 : (h + 1) * 128, :]
                    o = (-o if ri else o).astype(BF16)
                    wout[d, ri, h] = jnp.where(keep, dot(o, tiler), 0.0).astype(BF16)

    pr_ = iota((128, 128), 0)
    pc_ = iota((128, 128), 1)
    perm = (pc_ == lax.rem(pr_, 8) * 16 + pr_ // 8).astype(BF16)
    back = (pr_ == lax.rem(pc_, 8) * 16 + pc_ // 8).astype(BF16)
    u = [dot(perm, uw_ref[...]), dot(perm, un_ref[...])]
    ub = [x.astype(BF16) for x in u]
    for d in range(2):
        for s, win in enumerate((win_w, win_n)):
            n, first = SETS[s]
            for h in range(2):
                at = first + 8 * n * h
                for ri in range(2):
                    xs[d, ri, :, at : at + 8 * n] = dot(ub[s][:, h * 128 : (h + 1) * 128], win[d, ri, h])
    ef = jnp.concatenate(split3(jnp.exp(-forget_ref[...])), axis=0)
    ep = dot_nt(perm, ef).astype(BF16)
    sr = lax.rem(iota((192, NL), 0), 64)
    sc = iota((192, NL), 1)
    group_of = jnp.where(sc < 1024, sc // 64, 16 + (sc - 1024) // 32)
    for d in range(2):
        spread[d] = (sr == group_of + 32 * d).astype(BF16)
        es[d] = dot(ep, spread[d])

    def scan_step(i, state, c, keep_states):
        new = []
        for d in range(2):
            row = i if d == 0 else 15 - i
            at = pl.ds(pl.multiple_of(row * 8, 8), 8)
            lanes = slice(c * CHUNK, (c + 1) * CHUNK)
            lr = lam_ref[2 * d : 2 * d + 1, lanes]
            li = lam_ref[2 * d + 1 : 2 * d + 2, lanes]
            sre, sim = state[3 * d], state[3 * d + 1]
            e = es[d, at, lanes]
            nre = (lr * sre - li * sim) * e + xs[d, 0, at, lanes]
            nim = (lr * sim + li * sre) * e + xs[d, 1, at, lanes]
            if keep_states:
                xs[d, 0, at, lanes] = nre
                xs[d, 1, at, lanes] = nim
            new += [nre, nim, state[3 * d + 2] if keep_states else state[3 * d + 2] * e]
        return tuple(new)

    sub = iota((8, CHUNK), 0)
    ends = [[], []]
    for c in range(NL // CHUNK):
        zero = jnp.zeros((8, CHUNK), F32)
        one = jnp.ones((8, CHUNK), F32)
        state = lax.fori_loop(
            0, 16, lambda i, st: scan_step(i, st, c, False), (zero, zero, one, zero, zero, one)
        )
        lanes = slice(c * CHUNK, (c + 1) * CHUNK)
        for d in range(2):
            sre, sim, g = state[3 * d : 3 * d + 3]
            lr, li = lam_ref[2 * d : 2 * d + 1, lanes], lam_ref[2 * d + 1 : 2 * d + 2, lanes]
            for _ in range(4):
                lr, li = square(lr, li)
            place = sub if d == 0 else 7 - sub
            pre, pim = one, zero
            for k in (1, 2, 4):
                shift = k if d == 0 else 8 - k
                has = place >= k
                before_re = jnp.where(has, pltpu.roll(sre, shift, 0), 0.0) * g
                before_im = jnp.where(has, pltpu.roll(sim, shift, 0), 0.0) * g
                add_re, add_im = cmul(lr, li, before_re, before_im)
                sre, sim = sre + add_re, sim + add_im
                g = g * jnp.where(has, pltpu.roll(g, shift, 0), 1.0)
                tre, tim = cmul(lr, li, pre, pim)
                bit = lax.rem(place // k, 2) == 1
                pre, pim = jnp.where(bit, tre, pre), jnp.where(bit, tim, pim)
                lr, li = square(lr, li)
            edge = 7 if d == 0 else 0
            ends[d].append((sre[edge : edge + 1], sim[edge : edge + 1]))
            shift = 1 if d == 0 else 7
            has = place >= 1
            carry_ref[d, 0, :, lanes] = jnp.where(has, pltpu.roll(sre, shift, 0), 0.0)
            carry_ref[d, 1, :, lanes] = jnp.where(has, pltpu.roll(sim, shift, 0), 0.0)
            gx = jnp.where(has, pltpu.roll(g, shift, 0), 1.0)
            prod_ref[d, 0, :, lanes] = pre * gx
            prod_ref[d, 1, :, lanes] = pim * gx
            lam_ref[4 + 2 * d : 5 + 2 * d, lanes] = lr
            lam_ref[5 + 2 * d : 6 + 2 * d, lanes] = li

    fsum = lax.dot_general(
        jnp.ones((8, 128), F32), forget_ref[...], (((1,), (1,)), ((), ())),
        preferred_element_type=F32, precision=lax.Precision.HIGHEST,
    )[0:1]
    total = [
        [jnp.concatenate([e[q] for e in ends[d]], axis=1) for q in range(2)] for d in range(2)
    ]
    power = [[lam_ref[4 + 2 * d + q : 5 + 2 * d + q, :] for q in range(2)] for d in range(2)]
    enter = None
    pl.semaphore_wait(barrier, 10)
    for stage, a in enumerate(axes):
        p = pos[stage]
        for d in range(2):
            for q in range(2):
                r = 4 * d + 2 * q
                send[stage, r : r + 1, 0:768] = total[d][q][:, 0:768]
                send[stage, r + 1 : r + 2, 0:768] = total[d][q][:, 768:1536]
        send[stage, 0:1, 768:832] = fsum
        copies = []
        for o in (1, 3, 2):
            there = lax.rem(p + o, 4)
            copies.append(
                pltpu.make_async_remote_copy(
                    src_ref=send.at[stage],
                    dst_ref=recv.at[stage, p],
                    send_sem=send_sem.at[stage, o],
                    recv_sem=recv_sem.at[stage, p],
                    device_id={a: there},
                    device_id_type=MESH,
                )
            )
            copies[-1].start()
        for o in (1, 3, 2):
            there = lax.rem(p + o, 4)
            pltpu.make_async_remote_copy(
                src_ref=send.at[stage],
                dst_ref=recv.at[stage, there],
                send_sem=send_sem.at[stage, o],
                recv_sem=recv_sem.at[stage, there],
                device_id={a: there},
                device_id_type=MESH,
            ).wait_recv()
        recv[stage, p] = send[stage]
        sums = jnp.concatenate([recv[stage, k, 0:1, 768:832] for k in range(4)], axis=0)
        parts = jnp.concatenate(split3(jnp.exp(-sums)), axis=1)
        for d in range(2):
            g = dot(parts, spread[d])
            lr, li = power[d]
            rre = rim = jnp.zeros((1, NL), F32)
            ire = iim = jnp.zeros((1, NL), F32)
            are, aim = jnp.ones((1, NL), F32), jnp.zeros((1, NL), F32)
            jre, jim = are, aim
            for step in range(4):
                k = step if d == 0 else 3 - step
                here = k == p
                ire, iim = jnp.where(here, rre, ire), jnp.where(here, rim, iim)
                nearer = (k < p) if d == 0 else (k > p)
                gr, gi = lr * g[k : k + 1], li * g[k : k + 1]
                r = 4 * d
                tre = jnp.concatenate([recv[stage, k, r : r + 1, 0:768], recv[stage, k, r + 1 : r + 2, 0:768]], axis=1)
                tim = jnp.concatenate([recv[stage, k, r + 2 : r + 3, 0:768], recv[stage, k, r + 3 : r + 4, 0:768]], axis=1)
                rre, rim = cmul(gr, gi, rre, rim)
                rre, rim = rre + tre, rim + tim
                nre, nim = cmul(gr, gi, jre, jim)
                jre, jim = jnp.where(nearer, nre, jre), jnp.where(nearer, nim, jim)
            total[d] = [rre, rim]
            lr, li = square(*square(lr, li))
            power[d] = [lr, li]
            if enter is None or len(enter) < 2:
                enter = (enter or []) + [[ire, iim, jre, jim]]
            else:
                bre, bim, cre, cim = enter[d]
                add_re, add_im = cmul(cre, cim, ire, iim)
                ncre, ncim = cmul(cre, cim, jre, jim)
                enter[d] = [bre + add_re, bim + add_im, ncre, ncim]
        fsum = jnp.sum(sums, axis=0, keepdims=True)
        for copy in copies:
            copy.wait_send()

    for c in range(NL // CHUNK):
        lanes = slice(c * CHUNK, (c + 1) * CHUNK)
        state = []
        for d in range(2):
            cre, cim = enter[d][0][:, lanes], enter[d][1][:, lanes]
            add_re, add_im = cmul(prod_ref[d, 0, :, lanes], prod_ref[d, 1, :, lanes], cre, cim)
            state += [carry_ref[d, 0, :, lanes] + add_re, carry_ref[d, 1, :, lanes] + add_im, jnp.zeros((8, 128), F32)]
        lax.fori_loop(0, 16, lambda i, st: scan_step(i, st, c, True), tuple(state))

    for s, wout in enumerate((wout_w, wout_n)):
        n, first = SETS[s]
        for h in range(2):
            at = first + 8 * n * h
            y = None
            for d in range(2):
                for ri in range(2):
                    term = dot_nt(xs[d, ri, :, at : at + 8 * n].astype(BF16), wout[d, ri, h])
                    y = term if y is None else y + term
            ch = slice(h * 128, (h + 1) * 128)
            y = y + skip_ref[s : s + 1, ch].astype(F32) * u[s][:, ch]
            active = jax.nn.gelu(y, approximate=True)
            gr = iota((16, 128), 0)
            gc = iota((16, 128), 1)
            tiler = (gr == lax.rem(gc, 16)).astype(BF16)
            gate = dot(gate_ref[s, ch, :], tiler)
            gate = jnp.where(iota((128, 128), 0) // 16 == iota((128, 128), 1) // 16, gate, 0.0).astype(BF16)
            opened = jax.nn.sigmoid(dot(active.astype(BF16), gate))
            done = dot(back, (active * opened).astype(BF16)).astype(BF16)
            for half in range(2):
                mine[half, :, s * 256 + h * 128 : s * 256 + (h + 1) * 128] = done[half * 64 : (half + 1) * 64]

    copy = pltpu.make_async_remote_copy(
        src_ref=mine.at[1 - core],
        dst_ref=out_ref.at[core],
        send_sem=tp_send,
        recv_sem=tp_recv,
        device_id={"tp": 1 - core},
        device_id_type=MESH,
    )
    copy.start()
    out_ref[core] = mine[core]
    copy.wait()


def mixer(wide_inputs, narrow_inputs, wide_poles, narrow_poles, step_sizes, forget, wide_in_map,
          narrow_in_map, wide_out_map, narrow_out_map, skip_weight, gate_mix):
    vm = pl.BlockSpec(memory_space=pltpu.VMEM)
    return pl.pallas_call(
        mixer_kernel,
        out_shape=jax.ShapeDtypeStruct((2, 64, 512), BF16),
        in_specs=[vm] * 12,
        out_specs=vm,
        scratch_shapes=[
            pltpu.VMEM((2, 2, 2, 128, 512), BF16),
            pltpu.VMEM((2, 2, 2, 128, 256), BF16),
            pltpu.VMEM((2, 2, 2, 128, 512), BF16),
            pltpu.VMEM((2, 2, 2, 128, 256), BF16),
            pltpu.VMEM((2, 2, 128, NL), F32),
            pltpu.VMEM((2, 128, NL), F32),
            pltpu.VMEM((2, 192, NL), BF16),
            pltpu.VMEM((2, 2, 8, NL), F32),
            pltpu.VMEM((2, 2, 8, NL), F32),
            pltpu.VMEM((8, NL), F32),
            pltpu.VMEM((3, 8, 896), F32),
            pltpu.VMEM((3, 4, 8, 896), F32),
            pltpu.VMEM((2, 64, 512), BF16),
            pltpu.SemaphoreType.DMA((3, 4)),
            pltpu.SemaphoreType.DMA((3, 4)),
            pltpu.SemaphoreType.DMA,
            pltpu.SemaphoreType.DMA,
        ],
        compiler_params=pltpu.CompilerParams(
            collective_id=0, has_side_effects=True, vmem_limit_bytes=50 * 1024 * 1024
        ),
        name="mixer",
    )(
        wide_inputs, narrow_inputs, wide_poles, narrow_poles, step_sizes.reshape(2, 2, 16, 1),
        forget.reshape(64, 128),
        wide_in_map.reshape(2, 2, 256, 64), narrow_in_map.reshape(2, 2, 256, 32),
        wide_out_map.reshape(2, 2, 256, 64), narrow_out_map.reshape(2, 2, 256, 32),
        skip_weight, gate_mix.reshape(2, 256, 16),
    )


def in_blocks(shard, dim, count):
    dims = shard.shape
    blocks = shard.reshape(*dims[:dim], count, dims[dim] // count, *dims[dim + 1 :])
    return jnp.moveaxis(blocks, dim, 0)


def one_exchange(blocks):
    return lax.all_to_all(blocks, SP_TP, split_axis=0, concat_axis=0, tiled=True)


def local(
    wide_inputs, narrow_inputs, wide_poles, narrow_poles, step_sizes, forget, wide_in_map,
    narrow_in_map, wide_out_map, narrow_out_map, skip_weight, gate_mix, residual, mixer_gain,
    out_proj, ffn_gain, routes, route_weights, gate_proj, up_proj, down_proj,
):
    parts = mixer(wide_inputs, narrow_inputs, wide_poles, narrow_poles, step_sizes, forget,
                  wide_in_map, narrow_in_map, wide_out_map, narrow_out_map, skip_weight, gate_mix)
    joined = jnp.concatenate(
        [parts[0, :, :256], parts[1, :, :256], parts[0, :, 256:], parts[1, :, 256:]], axis=1
    ).astype(F32)
    scale = lax.rsqrt(jnp.mean(joined * joined, axis=1, keepdims=True) + epsilon)
    mixed = (joined * scale * mixer_gain).astype(BF16)
    projected = jnp.dot(mixed, out_proj, preferred_element_type=F32)
    hidden1 = (residual.astype(F32) + projected).astype(BF16)
    hidden_wide = hidden1.astype(F32)
    normed = (
        hidden_wide
        * lax.rsqrt(jnp.mean(hidden_wide * hidden_wide, axis=1, keepdims=True) + epsilon)
        * ffn_gain
    ).astype(BF16)
    experts, capacity = 128, 2
    width = normed.shape[1]
    picks = routes.reshape(-1)
    onehot = (picks[:, None] == jnp.arange(experts, dtype=jnp.int32)[None, :]).astype(jnp.int32)
    rank = jnp.sum((jnp.cumsum(onehot, axis=0) - onehot) * onehot, axis=1)
    place = picks * capacity + rank
    sectioning = (
        jnp.zeros((experts * capacity, width), BF16).at[place].set(jnp.repeat(normed, 2, axis=0))
    )
    flat_rows = one_exchange(sectioning)
    gate_val = jnp.dot(flat_rows, gate_proj[0], preferred_element_type=F32)
    up_val = jnp.dot(flat_rows, up_proj[0], preferred_element_type=F32)
    expert_hidden = (jax.nn.silu(gate_val) * up_val).astype(BF16)
    done = jnp.dot(expert_hidden, down_proj[0], preferred_element_type=F32).astype(BF16)
    returned = one_exchange(done)
    taken = jnp.take(returned, place, axis=0).reshape(-1, 2, width)
    share = route_weights / jnp.sum(route_weights, axis=1, keepdims=True)
    result = hidden_wide + jnp.sum(share[:, :, None] * taken.astype(F32), axis=1)
    return result.astype(BF16)


def solution(mesh):
    finer = Mesh(mesh.devices.reshape(4, 4, 4, mesh.shape["tp"]), ("sp_0", "sp_1", "sp_2", "tp"))
    return jax.shard_map(
        local,
        mesh=finer,
        in_specs=(
            P(SP, "tp"),
            P(SP, "tp"),
            P(None, None, "tp", None),
            P(None, None, "tp", None),
            P(None, None, "tp"),
            P(None, None, "tp", SP),
            P(None, None, "tp", None, None),
            P(None, None, "tp", None, None),
            P(None, None, "tp", None, None),
            P(None, None, "tp", None, None),
            P(None, "tp"),
            P(None, "tp", None, None),
            P(SP_TP, None),
            P(),
            P(),
            P(),
            P(SP_TP, None),
            P(SP_TP, None),
            P(SP_TP, None, None),
            P(SP_TP, None, None),
            P(SP_TP, None, None),
        ),
        out_specs=P(SP_TP, None),
        check_vma=False,
    )
```

```python
import functools

import jax
import jax.numpy as jnp
from jax import lax
from jax.experimental import pallas as pl
from jax.experimental.pallas import tpu as pltpu
from jax.sharding import Mesh
from jax.sharding import PartitionSpec as P

SP = ("sp_0", "sp_1", "sp_2")
SP_TP = ("sp_0", "sp_1", "sp_2", "tp")
MESH = pl.DeviceIdType.MESH
epsilon = 1e-06
F32 = jnp.float32
BF16 = jnp.bfloat16
NL = 1536
SETS = ((64, 0), (32, 1024))
CHUNK = 512


def dot(a, b):
    return lax.dot_general(a, b, (((1,), (0,)), ((), ())), preferred_element_type=F32)


def dot_nt(a, b):
    return lax.dot_general(a, b, (((1,), (1,)), ((), ())), preferred_element_type=F32)


def split3(x):
    first = x.astype(BF16)
    rest = x - first.astype(F32)
    second = rest.astype(BF16)
    third = (rest - second.astype(F32)).astype(BF16)
    return first, second, third


def iota(shape, dim):
    return lax.broadcasted_iota(jnp.int32, shape, dim)


def cmul(ar, ai, br, bi):
    return ar * br - ai * bi, ar * bi + ai * br


def square(ar, ai):
    return ar * ar - ai * ai, 2.0 * ar * ai


def coords():
    return [lax.axis_index(a) for a in SP_TP]


def partner(o):
    o = lax.rem(o * 37, 128)
    steps = (o // 32, lax.rem(o // 8, 4), lax.rem(o // 2, 4), lax.rem(o, 2))
    there = [lax.rem(p + s, n) for p, s, n in zip(coords(), steps, (4, 4, 4, 2))]
    number = ((there[0] * 4 + there[1]) * 4 + there[2]) * 2 + there[3]
    return dict(zip(SP_TP, there)), number


def my_number():
    z, y, x, c = coords()
    return ((z * 4 + y) * 4 + x) * 2 + c


def to_everyone(out, arrived, send_sem, recv_sem):
    me = my_number()

    def one(o, carry):
        where, number = partner(o)
        pltpu.make_async_remote_copy(
            src_ref=out.at[number], dst_ref=arrived.at[me], send_sem=send_sem, recv_sem=recv_sem,
            device_id=where, device_id_type=MESH,
        ).start()
        return carry

    lax.fori_loop(1, 128, one, 0)
    arrived[me] = out[me]


def all_of(out, arrived, send_sem, recv_sem):
    return pltpu.make_async_remote_copy(
        src_ref=out.at[pl.ds(0, 127)], dst_ref=arrived.at[pl.ds(0, 127)], send_sem=send_sem,
        recv_sem=recv_sem, device_id={"tp": 1 - lax.axis_index("tp")}, device_id_type=MESH,
    )


def swap_matrix():
    r, c = iota((256, 256), 0), iota((256, 256), 1)
    return (lax.rem(r, 16) * 16 + r // 16 == c).astype(BF16)


def pack(rows, swap, out):
    for k in range(4):
        both = jnp.concatenate(
            [
                jnp.concatenate(
                    [rows(q // 8, 16 * (2 * k + side), q % 8) for q in range(16)], axis=0
                )
                for side in range(2)
            ],
            axis=1,
        )
        done = dot(swap, both).astype(BF16)
        for side in range(2):
            at = 16 * (2 * k + side)
            out[at : at + 16] = done[:, side * 128 : (side + 1) * 128].reshape(16, 16, 128)


def unpack(block, swap, put):
    for k in range(4):
        both = jnp.concatenate(
            [block(16 * (2 * k + side)).reshape(256, 128) for side in range(2)], axis=1
        )
        done = dot(swap, both).astype(BF16)
        for side in range(2):
            at = 16 * (2 * k + side)
            for q in range(16):
                put(q // 8, at, q % 8, done[q * 16 : (q + 1) * 16, side * 128 : (side + 1) * 128])


def layer_kernel(*refs):
    ins, out_ref, held = refs[:21], refs[21], refs[22 : 22 + 21]
    (win_w, win_n, wout_w, wout_n, xs, es, spread, carry_ref, prod_ref, lam_ref, send, recv, mine, theirs,
     res_out, res_in, mix_out, mix_in, ret_out, ret_in, slots, rows_ref, mixed_ref, hidden_ref, normed_ref, inner_ref,
     back_ref, own_ref,
     load_sem, send_sem, recv_sem, tp_send, tp_recv, all_send, all_recv) = refs[43:]
    axes = ("sp_2", "sp_1", "sp_0")
    pos = [lax.axis_index(a) for a in axes]
    core = lax.axis_index("tp")

    barrier = pltpu.get_barrier_semaphore()

    def greet(o, carry):
        where, _ = partner(o)
        pl.semaphore_signal(barrier, inc=1, device_id=where, device_id_type=MESH)
        return carry

    lax.fori_loop(1, 128, greet, 0)
    loads = [pltpu.make_async_copy(a, b, load_sem.at[k]) for k, (a, b) in enumerate(zip(ins, held))]
    order = [12, 16, 2, 3, 4, 6, 7, 8, 9, 0, 1, 5, 10, 11, 13, 15, 17, 14, 18, 19, 20]
    for k in order:
        loads[k].start()
    (uw_ref, un_ref, pw_ref, pn_ref, step_ref, forget_ref, inw_ref, inn_ref, ow_ref, on_ref,
     skip_ref, gate_ref, residual_ref, mgain_ref, outp_ref, fgain_ref, routes_ref, weights_ref,
     wg_ref, wu_ref, wd_ref) = held
    for k in order[:2]:
        loads[k].wait()

    swap = swap_matrix()
    earlier = (iota((64, 64), 0) < iota((64, 64), 1)).astype(BF16)
    named = [(iota((128, 64), 0) == routes_ref[k : k + 1, :]).astype(F32) for k in range(2)]
    count = named[0] + named[1]
    rank = dot(count.astype(BF16), earlier)
    pick = [jnp.where(rank == r, count, 0.0).astype(BF16) for r in range(2)]
    for half in range(2):
        for r in range(2):
            slots[r] = dot(pick[r], residual_ref[:, half * 1024 : (half + 1) * 1024]).astype(BF16)
        pack(lambda r, at, j: slots[r, at : at + 16, j * 128 : (j + 1) * 128], swap, res_out.at[half])
    pl.semaphore_wait(barrier, 127)
    for half in range(2):
        to_everyone(res_out.at[half], res_in.at[half], all_send.at[half], all_recv.at[half])
    for k in order[2:14]:
        loads[k].wait()

    for s, (p_ref, in_ref, o_ref, win, wout) in enumerate(
        ((pw_ref, inw_ref, ow_ref, win_w, wout_w), (pn_ref, inn_ref, on_ref, win_n, wout_n))
    ):
        n, first = SETS[s]
        tile_r = iota((n, 8 * n), 0)
        tile_c = iota((n, 8 * n), 1)
        tiler = (tile_r == lax.rem(tile_c, n)).astype(BF16)
        wr = iota((128, 8 * n), 0)
        wc = iota((128, 8 * n), 1)
        keep = (wr // 16) == (wc // n)
        for d in range(2):
            pr = p_ref[d, 0]
            pi = p_ref[d, 1]
            grow = jnp.exp(pr)
            lre = grow * jnp.cos(pi)
            lim = grow * jnp.sin(pi)
            nre = lre - 1.0
            step = jnp.sum(jnp.where(iota((16, 16), 0) == iota((16, 16), 1), step_ref[d, s : s + 1, :], 0.0), axis=1, keepdims=True)
            scale = step / (pr * pr + pi * pi)
            fre = (nre * pr + lim * pi) * scale
            fim = (lim * pr - nre * pi) * scale
            for ri, lam in ((0, lre), (1, lim)):
                parts = jnp.concatenate(split3(lam), axis=0)
                for h in range(2):
                    wide = dot(parts, tiler)
                    gr = lax.rem(iota((48, 8 * n), 0), 16)
                    gc = iota((48, 8 * n), 1) // n + 8 * h
                    row = jnp.sum(jnp.where(gr == gc, wide, 0.0), axis=0, keepdims=True)
                    lam_ref[2 * d + ri : 2 * d + ri + 1, first + 8 * n * h : first + 8 * n * (h + 1)] = row
            ere, eim = [], []
            for g in range(16):
                a = in_ref[d, 0, g * 16 : (g + 1) * 16, :]
                b = in_ref[d, 1, g * 16 : (g + 1) * 16, :]
                fr, fi = fre[g : g + 1], fim[g : g + 1]
                ere.append((fr * a - fi * b).astype(BF16))
                eim.append((fr * b + fi * a).astype(BF16))
            for h in range(2):
                for ri, rows in ((0, ere), (1, eim)):
                    part = jnp.concatenate(rows[8 * h : 8 * h + 8], axis=0)
                    win[d, ri, h] = jnp.where(keep, dot(part, tiler), 0.0).astype(BF16)
                    o = o_ref[d, ri, h * 128 : (h + 1) * 128, :]
                    o = (-o if ri else o).astype(BF16)
                    wout[d, ri, h] = jnp.where(keep, dot(o, tiler), 0.0).astype(BF16)

    pr_ = iota((128, 128), 0)
    pc_ = iota((128, 128), 1)
    perm = (pc_ == lax.rem(pr_, 8) * 16 + pr_ // 8).astype(BF16)
    back = (pr_ == lax.rem(pc_, 8) * 16 + pc_ // 8).astype(BF16)
    u = [dot(perm, uw_ref[...]), dot(perm, un_ref[...])]
    ub = [x.astype(BF16) for x in u]
    for d in range(2):
        for s, win in enumerate((win_w, win_n)):
            n, first = SETS[s]
            for h in range(2):
                at = first + 8 * n * h
                for ri in range(2):
                    xs[d, ri, :, at : at + 8 * n] = dot(ub[s][:, h * 128 : (h + 1) * 128], win[d, ri, h])
    ef = jnp.concatenate(split3(jnp.exp(-forget_ref[...])), axis=0)
    ep = dot_nt(perm, ef).astype(BF16)
    sr = lax.rem(iota((192, NL), 0), 64)
    sc = iota((192, NL), 1)
    group_of = jnp.where(sc < 1024, sc // 64, 16 + (sc - 1024) // 32)
    for d in range(2):
        spread[d] = (sr == group_of + 32 * d).astype(BF16)
        es[d] = dot(ep, spread[d])

    def scan_step(i, state, c, keep_states):
        new = []
        for d in range(2):
            row = i if d == 0 else 15 - i
            at = pl.ds(pl.multiple_of(row * 8, 8), 8)
            lanes = slice(c * CHUNK, (c + 1) * CHUNK)
            lr = lam_ref[2 * d : 2 * d + 1, lanes]
            li = lam_ref[2 * d + 1 : 2 * d + 2, lanes]
            sre, sim = state[3 * d], state[3 * d + 1]
            e = es[d, at, lanes]
            nre = (lr * sre - li * sim) * e + xs[d, 0, at, lanes]
            nim = (lr * sim + li * sre) * e + xs[d, 1, at, lanes]
            if keep_states:
                xs[d, 0, at, lanes] = nre
                xs[d, 1, at, lanes] = nim
            new += [nre, nim, state[3 * d + 2] if keep_states else state[3 * d + 2] * e]
        return tuple(new)

    sub = iota((8, CHUNK), 0)
    ends = [[], []]
    for c in range(NL // CHUNK):
        zero = jnp.zeros((8, CHUNK), F32)
        one = jnp.ones((8, CHUNK), F32)
        state = lax.fori_loop(
            0, 16, lambda i, st: scan_step(i, st, c, False), (zero, zero, one, zero, zero, one)
        )
        lanes = slice(c * CHUNK, (c + 1) * CHUNK)
        for d in range(2):
            sre, sim, g = state[3 * d : 3 * d + 3]
            lr, li = lam_ref[2 * d : 2 * d + 1, lanes], lam_ref[2 * d + 1 : 2 * d + 2, lanes]
            for _ in range(4):
                lr, li = square(lr, li)
            place = sub if d == 0 else 7 - sub
            pre, pim = one, zero
            for k in (1, 2, 4):
                shift = k if d == 0 else 8 - k
                has = place >= k
                before_re = jnp.where(has, pltpu.roll(sre, shift, 0), 0.0) * g
                before_im = jnp.where(has, pltpu.roll(sim, shift, 0), 0.0) * g
                add_re, add_im = cmul(lr, li, before_re, before_im)
                sre, sim = sre + add_re, sim + add_im
                g = g * jnp.where(has, pltpu.roll(g, shift, 0), 1.0)
                tre, tim = cmul(lr, li, pre, pim)
                bit = lax.rem(place // k, 2) == 1
                pre, pim = jnp.where(bit, tre, pre), jnp.where(bit, tim, pim)
                lr, li = square(lr, li)
            edge = 7 if d == 0 else 0
            ends[d].append((sre[edge : edge + 1], sim[edge : edge + 1]))
            shift = 1 if d == 0 else 7
            has = place >= 1
            carry_ref[d, 0, :, lanes] = jnp.where(has, pltpu.roll(sre, shift, 0), 0.0)
            carry_ref[d, 1, :, lanes] = jnp.where(has, pltpu.roll(sim, shift, 0), 0.0)
            gx = jnp.where(has, pltpu.roll(g, shift, 0), 1.0)
            prod_ref[d, 0, :, lanes] = pre * gx
            prod_ref[d, 1, :, lanes] = pim * gx
            lam_ref[4 + 2 * d : 5 + 2 * d, lanes] = lr
            lam_ref[5 + 2 * d : 6 + 2 * d, lanes] = li

    fsum = lax.dot_general(
        jnp.ones((8, 128), F32), forget_ref[...], (((1,), (1,)), ((), ())),
        preferred_element_type=F32, precision=lax.Precision.HIGHEST,
    )[0:1]
    total = [
        [jnp.concatenate([e[q] for e in ends[d]], axis=1) for q in range(2)] for d in range(2)
    ]
    power = [[lam_ref[4 + 2 * d + q : 5 + 2 * d + q, :] for q in range(2)] for d in range(2)]
    enter = None
    for stage, a in enumerate(axes):
        p = pos[stage]
        for d in range(2):
            for q in range(2):
                r = 4 * d + 2 * q
                send[stage, r : r + 1, 0:768] = total[d][q][:, 0:768]
                send[stage, r + 1 : r + 2, 0:768] = total[d][q][:, 768:1536]
        send[stage, 0:1, 768:832] = fsum
        copies = []
        for o in (1, 3, 2):
            there = lax.rem(p + o, 4)
            copies.append(
                pltpu.make_async_remote_copy(
                    src_ref=send.at[stage],
                    dst_ref=recv.at[stage, p],
                    send_sem=send_sem.at[stage, o],
                    recv_sem=recv_sem.at[stage, p],
                    device_id={a: there},
                    device_id_type=MESH,
                )
            )
            copies[-1].start()
        for o in (1, 3, 2):
            there = lax.rem(p + o, 4)
            pltpu.make_async_remote_copy(
                src_ref=send.at[stage],
                dst_ref=recv.at[stage, there],
                send_sem=send_sem.at[stage, o],
                recv_sem=recv_sem.at[stage, there],
                device_id={a: there},
                device_id_type=MESH,
            ).wait_recv()
        recv[stage, p] = send[stage]
        sums = jnp.concatenate([recv[stage, k, 0:1, 768:832] for k in range(4)], axis=0)
        parts = jnp.concatenate(split3(jnp.exp(-sums)), axis=1)
        for d in range(2):
            g = dot(parts, spread[d])
            lr, li = power[d]
            rre = rim = jnp.zeros((1, NL), F32)
            ire = iim = jnp.zeros((1, NL), F32)
            are, aim = jnp.ones((1, NL), F32), jnp.zeros((1, NL), F32)
            jre, jim = are, aim
            for step in range(4):
                k = step if d == 0 else 3 - step
                here = k == p
                ire, iim = jnp.where(here, rre, ire), jnp.where(here, rim, iim)
                nearer = (k < p) if d == 0 else (k > p)
                gr, gi = lr * g[k : k + 1], li * g[k : k + 1]
                r = 4 * d
                tre = jnp.concatenate([recv[stage, k, r : r + 1, 0:768], recv[stage, k, r + 1 : r + 2, 0:768]], axis=1)
                tim = jnp.concatenate([recv[stage, k, r + 2 : r + 3, 0:768], recv[stage, k, r + 3 : r + 4, 0:768]], axis=1)
                rre, rim = cmul(gr, gi, rre, rim)
                rre, rim = rre + tre, rim + tim
                nre, nim = cmul(gr, gi, jre, jim)
                jre, jim = jnp.where(nearer, nre, jre), jnp.where(nearer, nim, jim)
            total[d] = [rre, rim]
            lr, li = square(*square(lr, li))
            power[d] = [lr, li]
            if enter is None or len(enter) < 2:
                enter = (enter or []) + [[ire, iim, jre, jim]]
            else:
                bre, bim, cre, cim = enter[d]
                add_re, add_im = cmul(cre, cim, ire, iim)
                ncre, ncim = cmul(cre, cim, jre, jim)
                enter[d] = [bre + add_re, bim + add_im, ncre, ncim]
        fsum = jnp.sum(sums, axis=0, keepdims=True)
        for copy in copies:
            copy.wait_send()

    for c in range(NL // CHUNK):
        lanes = slice(c * CHUNK, (c + 1) * CHUNK)
        state = []
        for d in range(2):
            cre, cim = enter[d][0][:, lanes], enter[d][1][:, lanes]
            add_re, add_im = cmul(prod_ref[d, 0, :, lanes], prod_ref[d, 1, :, lanes], cre, cim)
            state += [carry_ref[d, 0, :, lanes] + add_re, carry_ref[d, 1, :, lanes] + add_im, jnp.zeros((8, 128), F32)]
        lax.fori_loop(0, 16, lambda i, st: scan_step(i, st, c, True), tuple(state))

    for s, wout in enumerate((wout_w, wout_n)):
        n, first = SETS[s]
        for h in range(2):
            at = first + 8 * n * h
            y = None
            for d in range(2):
                for ri in range(2):
                    term = dot_nt(xs[d, ri, :, at : at + 8 * n].astype(BF16), wout[d, ri, h])
                    y = term if y is None else y + term
            ch = slice(h * 128, (h + 1) * 128)
            y = y + skip_ref[s : s + 1, ch].astype(F32) * u[s][:, ch]
            active = jax.nn.gelu(y, approximate=True)
            gr = iota((16, 128), 0)
            gc = iota((16, 128), 1)
            tiler = (gr == lax.rem(gc, 16)).astype(BF16)
            gate = dot(gate_ref[s, ch, :], tiler)
            gate = jnp.where(iota((128, 128), 0) // 16 == iota((128, 128), 1) // 16, gate, 0.0).astype(BF16)
            opened = jax.nn.sigmoid(dot(active.astype(BF16), gate))
            done = dot(back, (active * opened).astype(BF16)).astype(BF16)
            for half in range(2):
                mine[half, :, s * 256 + h * 128 : s * 256 + (h + 1) * 128] = done[half * 64 : (half + 1) * 64]

    copy = pltpu.make_async_remote_copy(
        src_ref=mine.at[1 - core],
        dst_ref=theirs,
        send_sem=tp_send,
        recv_sem=tp_recv,
        device_id={"tp": 1 - core},
        device_id_type=MESH,
    )
    copy.start()
    for k in order[14:18]:
        loads[k].wait()
    copy.wait()

    own, other = mine[core].astype(F32), theirs[...].astype(F32)
    low = jnp.where(core == 0, own, other)
    high = jnp.where(core == 0, other, own)
    joined = jnp.concatenate([low[:, :256], high[:, :256], low[:, 256:], high[:, 256:]], axis=1)
    scale = lax.rsqrt(jnp.mean(joined * joined, axis=1, keepdims=True) + epsilon)
    mixed = (joined * scale * mgain_ref[...]).astype(BF16)
    for r in range(2):
        slots[r] = dot(pick[r], mixed).astype(BF16)
    pack(lambda r, at, j: slots[r, at : at + 16, j * 128 : (j + 1) * 128], swap, mix_out)
    to_everyone(mix_out, mix_in, all_send.at[2], all_recv.at[2])

    for c in range(8):
        lanes = slice(c * 256, (c + 1) * 256)
        own_ref[:, lanes] = (
            residual_ref[:, lanes].astype(F32) + dot(mixed, outp_ref[:, lanes])
        ).astype(BF16)
    for half in range(2):
        all_of(res_out.at[half], res_in.at[half], all_send.at[half], all_recv.at[half]).wait_recv()

        def put(r, at, j, rows):
            lanes = half * 1024 + j * 128
            rows_ref[r * 128 + at : r * 128 + at + 16, lanes : lanes + 128] = rows

        unpack(lambda at: res_in[half, at : at + 16], swap, put)

    eye = iota((64, 64), 0) == iota((64, 64), 1)
    def column(row):
        return jnp.sum(jnp.where(eye, row, 0.0), axis=1, keepdims=True)
    experts = iota((64, 128), 1).astype(F32)
    hits = [(column(routes_ref[k : k + 1, :].astype(F32)) == experts).astype(F32) for k in range(2)]
    w = [column(weights_ref[k : k + 1, :]) for k in range(2)]
    both = w[0] + w[1]
    before = (iota((64, 64), 1) < iota((64, 64), 0)).astype(BF16)
    ranks = dot(before, (hits[0] + hits[1]).astype(BF16))
    shares = hits[0] * (w[0] / both) + hits[1] * (w[1] / both)
    parts = []
    for r in range(2):
        share = jnp.where(ranks == r, shares, 0.0)
        first = share.astype(BF16)
        parts.append((first, (share - first.astype(F32)).astype(BF16)))

    for k in order[18:]:
        loads[k].wait()
    all_of(mix_out, mix_in, all_send.at[2], all_recv.at[2]).wait_recv()

    def put_mixed(r, at, j, rows):
        mixed_ref[r * 128 + at : r * 128 + at + 16, j * 128 : (j + 1) * 128] = rows

    unpack(lambda at: mix_in[at : at + 16], swap, put_mixed)
    square_sum = jnp.zeros((256, 1), F32)
    for c in range(8):
        lanes = slice(c * 256, (c + 1) * 256)
        h = (rows_ref[:, lanes].astype(F32) + dot(mixed_ref[...], outp_ref[:, lanes])).astype(BF16)
        hidden_ref[:, lanes] = h
        wide = h.astype(F32)
        square_sum = square_sum + jnp.sum(wide * wide, axis=1, keepdims=True)
    scale = lax.rsqrt(square_sum / 2048.0 + epsilon)
    for c in range(8):
        lanes = slice(c * 256, (c + 1) * 256)
        normed_ref[:, lanes] = (hidden_ref[:, lanes].astype(F32) * scale * fgain_ref[:, lanes]).astype(BF16)

    def expert_step(lanes):
        g = dot(normed_ref[...], wg_ref[0, :, lanes])
        v = dot(normed_ref[...], wu_ref[0, :, lanes])
        inner_ref[:, lanes] = (jax.nn.silu(g) * v).astype(BF16)

    for c in range(5):
        expert_step(slice(c * 256, (c + 1) * 256))
    expert_step(slice(1280, 1408))

    for half in range(2):
        for c in range(4):
            lanes = slice(half * 1024 + c * 256, half * 1024 + (c + 1) * 256)
            y = dot(inner_ref[...], wd_ref[0, :, lanes]).astype(BF16)
            for r in range(2):
                slots[r, :, c * 256 : (c + 1) * 256] = y[r * 128 : (r + 1) * 128]
        pack(lambda r, at, j: slots[r, at : at + 16, j * 128 : (j + 1) * 128], swap, ret_out.at[half])
        to_everyone(ret_out.at[half], ret_in.at[half], all_send.at[3 + half], all_recv.at[3 + half])

    for half in range(2):
        all_of(ret_out.at[half], ret_in.at[half], all_send.at[3 + half], all_recv.at[3 + half]).wait_recv()

        def put_back(r, at, j, rows):
            back_ref[r, at : at + 16, j * 128 : (j + 1) * 128] = rows

        unpack(lambda at: ret_in[half, at : at + 16], swap, put_back)
        for c in range(4):
            lanes = slice(c * 256, (c + 1) * 256)
            to = slice(half * 1024 + c * 256, half * 1024 + (c + 1) * 256)
            y = None
            for r in range(2):
                for part in parts[r]:
                    term = dot(part, back_ref[r, :, lanes])
                    y = term if y is None else y + term
            out_ref[:, to] = (own_ref[:, to].astype(F32) + y).astype(BF16)

    for half in range(2):
        all_of(res_out.at[half], res_in.at[half], all_send.at[half], all_recv.at[half]).wait_send()
        all_of(ret_out.at[half], ret_in.at[half], all_send.at[3 + half], all_recv.at[3 + half]).wait_send()
    all_of(mix_out, mix_in, all_send.at[2], all_recv.at[2]).wait_send()


def local(
    wide_inputs, narrow_inputs, wide_poles, narrow_poles, step_sizes, forget, wide_in_map,
    narrow_in_map, wide_out_map, narrow_out_map, skip_weight, gate_mix, residual, mixer_gain,
    out_proj, ffn_gain, routes, route_weights, gate_proj, up_proj, down_proj,
):
    ins = (
        wide_inputs, narrow_inputs, wide_poles, narrow_poles, step_sizes, forget.reshape(64, 128),
        wide_in_map.reshape(2, 2, 256, 64), narrow_in_map.reshape(2, 2, 256, 32),
        wide_out_map.reshape(2, 2, 256, 64), narrow_out_map.reshape(2, 2, 256, 32),
        skip_weight, gate_mix.reshape(2, 256, 16), residual, mixer_gain.reshape(1, 1024), out_proj,
        ffn_gain.reshape(1, 2048), routes.T, route_weights.T, gate_proj, up_proj, down_proj,
    )
    scratch = [pltpu.VMEM(a.shape, a.dtype) for a in ins]
    scratch += [
        pltpu.VMEM((2, 2, 2, 128, 512), BF16),
        pltpu.VMEM((2, 2, 2, 128, 256), BF16),
        pltpu.VMEM((2, 2, 2, 128, 512), BF16),
        pltpu.VMEM((2, 2, 2, 128, 256), BF16),
        pltpu.VMEM((2, 2, 128, NL), F32),
        pltpu.VMEM((2, 128, NL), F32),
        pltpu.VMEM((2, 192, NL), BF16),
        pltpu.VMEM((2, 2, 8, NL), F32),
        pltpu.VMEM((2, 2, 8, NL), F32),
        pltpu.VMEM((8, NL), F32),
        pltpu.VMEM((3, 8, 896), F32),
        pltpu.VMEM((3, 4, 8, 896), F32),
        pltpu.VMEM((2, 64, 512), BF16),
        pltpu.VMEM((64, 512), BF16),
        pltpu.VMEM((2, 128, 16, 128), BF16),
        pltpu.VMEM((2, 128, 16, 128), BF16),
        pltpu.VMEM((128, 16, 128), BF16),
        pltpu.VMEM((128, 16, 128), BF16),
        pltpu.VMEM((2, 128, 16, 128), BF16),
        pltpu.VMEM((2, 128, 16, 128), BF16),
        pltpu.VMEM((2, 128, 1024), BF16),
        pltpu.VMEM((256, 2048), BF16),
        pltpu.VMEM((256, 1024), BF16),
        pltpu.VMEM((256, 2048), BF16),
        pltpu.VMEM((256, 2048), BF16),
        pltpu.VMEM((256, 1408), BF16),
        pltpu.VMEM((2, 128, 1024), BF16),
        pltpu.VMEM((64, 2048), BF16),
        pltpu.SemaphoreType.DMA((21,)),
        pltpu.SemaphoreType.DMA((3, 4)),
        pltpu.SemaphoreType.DMA((3, 4)),
        pltpu.SemaphoreType.DMA,
        pltpu.SemaphoreType.DMA,
        pltpu.SemaphoreType.DMA((5,)),
        pltpu.SemaphoreType.DMA((5,)),
    ]
    return pl.pallas_call(
        layer_kernel,
        out_shape=jax.ShapeDtypeStruct((64, 2048), BF16),
        in_specs=[pl.BlockSpec(memory_space=pl.ANY)] * 21,
        out_specs=pl.BlockSpec(memory_space=pltpu.VMEM),
        scratch_shapes=scratch,
        compiler_params=pltpu.CompilerParams(
            collective_id=0, has_side_effects=True, vmem_limit_bytes=60 * 1024 * 1024
        ),
        name="layer",
    )(*ins)


def solution(mesh):
    finer = Mesh(mesh.devices.reshape(4, 4, 4, mesh.shape["tp"]), ("sp_0", "sp_1", "sp_2", "tp"))
    return jax.shard_map(
        local,
        mesh=finer,
        in_specs=(
            P(SP, "tp"),
            P(SP, "tp"),
            P(None, None, "tp", None),
            P(None, None, "tp", None),
            P(None, None, "tp"),
            P(None, None, "tp", SP),
            P(None, None, "tp", None, None),
            P(None, None, "tp", None, None),
            P(None, None, "tp", None, None),
            P(None, None, "tp", None, None),
            P(None, "tp"),
            P(None, "tp", None, None),
            P(SP_TP, None),
            P(),
            P(),
            P(),
            P(SP_TP, None),
            P(SP_TP, None),
            P(SP_TP, None, None),
            P(SP_TP, None, None),
            P(SP_TP, None, None),
        ),
        out_specs=P(SP_TP, None),
        check_vma=False,
    )
```

```python
import functools

import jax
import jax.numpy as jnp
from jax import lax
from jax.experimental import pallas as pl
from jax.experimental.pallas import tpu as pltpu
from jax.sharding import Mesh
from jax.sharding import PartitionSpec as P

SP = ("sp_0", "sp_1", "sp_2")
SP_TP = ("sp_0", "sp_1", "sp_2", "tp")
MESH = pl.DeviceIdType.MESH
epsilon = 1e-06
F32 = jnp.float32
BF16 = jnp.bfloat16
NL = 1536
SETS = ((64, 0), (32, 1024))
CHUNK = 512
BATCHES = ((1, 31), (31, 61), (61, 91), (91, 128))
PARTS = ((0, 64), (64, 128))


def dot(a, b):
    return lax.dot_general(a, b, (((1,), (0,)), ((), ())), preferred_element_type=F32)


def dot_nt(a, b):
    return lax.dot_general(a, b, (((1,), (1,)), ((), ())), preferred_element_type=F32)


def split3(x):
    first = x.astype(BF16)
    rest = x - first.astype(F32)
    second = rest.astype(BF16)
    third = (rest - second.astype(F32)).astype(BF16)
    return first, second, third


def iota(shape, dim):
    return lax.broadcasted_iota(jnp.int32, shape, dim)


def cmul(ar, ai, br, bi):
    return ar * br - ai * bi, ar * bi + ai * br


def square(ar, ai):
    return ar * ar - ai * ai, 2.0 * ar * ai


def coords():
    return [lax.axis_index(a) for a in SP_TP]


def partner(o, way=1):
    o = lax.rem(o * 37, 128)
    steps = (o // 32, lax.rem(o // 8, 4), lax.rem(o // 2, 4), lax.rem(o, 2))
    sizes = (4, 4, 4, 2)
    there = [lax.rem(p + n + way * s, n) for p, s, n in zip(coords(), steps, sizes)]
    number = ((there[0] * 4 + there[1]) * 4 + there[2]) * 2 + there[3]
    return dict(zip(SP_TP, there)), number


def send_some(first, last, out, arrived, send_sem, recv_sem):
    def one(o, carry):
        where, _ = partner(o)
        pltpu.make_async_remote_copy(
            src_ref=out.at[o], dst_ref=arrived.at[o], send_sem=send_sem, recv_sem=recv_sem,
            device_id=where, device_id_type=MESH,
        ).start()
        return carry

    lax.fori_loop(first, last, one, 0)


def send_back(first, last, out, arrived, send_sem, recv_sem):
    def one(o, carry):
        where, _ = partner(o, -1)
        pltpu.make_async_remote_copy(
            src_ref=out.at[o], dst_ref=arrived.at[o], send_sem=send_sem, recv_sem=recv_sem,
            device_id=where, device_id_type=MESH,
        ).start()
        return carry

    lax.fori_loop(first, last, one, 0)


def all_of(first, last, out, arrived, send_sem, recv_sem):
    return pltpu.make_async_remote_copy(
        src_ref=out.at[pl.ds(first, last - first)], dst_ref=arrived.at[pl.ds(first, last - first)],
        send_sem=send_sem, recv_sem=recv_sem, device_id={"tp": 1 - lax.axis_index("tp")},
        device_id_type=MESH,
    )


def swap_matrix():
    r, c = iota((256, 256), 0), iota((256, 256), 1)
    return (lax.rem(r, 16) * 16 + r // 16 == c).astype(BF16)


def pack(rows, swap, put, blocks):
    for k in range(0, blocks, 32):
        both = jnp.concatenate(
            [
                jnp.concatenate([rows(q // 8, k + 16 * side, q % 8) for q in range(16)], axis=0)
                for side in range(2)
            ],
            axis=1,
        )
        done = dot(swap, both).astype(BF16)
        for side in range(2):
            put(k + 16 * side, done[:, side * 128 : (side + 1) * 128].reshape(16, 16, 128))


def unpack(block, swap, put, blocks):
    for k in range(0, blocks, 32):
        both = jnp.concatenate(
            [block(k + 16 * side).reshape(256, 128) for side in range(2)], axis=1
        )
        done = dot(swap, both).astype(BF16)
        for side in range(2):
            for q in range(16):
                put(q // 8, k + 16 * side, q % 8, done[q * 16 : (q + 1) * 16, side * 128 : (side + 1) * 128])


def layer_kernel(*refs):
    ins, out_ref, held = refs[:21], refs[21], refs[22 : 22 + 21]
    (win_w, win_n, wout_w, wout_n, xs, es, spread, carry_ref, prod_ref, lam_ref, send, recv, mine, theirs,
     res_out, res_in, mix_out, mix_in, ret_out, ret_in, slots, rows_ref, mixed_ref, hidden_ref, normed_ref, inner_ref,
     back_ref, own_ref,
     load_sem, send_sem, recv_sem, tp_send, tp_recv, all_send, all_recv, known_sem) = refs[43:]
    axes = ("sp_2", "sp_1", "sp_0")
    pos = [lax.axis_index(a) for a in axes]
    core = lax.axis_index("tp")

    barrier = pltpu.get_barrier_semaphore()

    def greet(semaphore, axis, place, size):
        for o in range(1, size):
            pl.semaphore_signal(semaphore, inc=1, device_id={axis: lax.rem(place + o, size)}, device_id_type=MESH)

    for a, p in zip(axes, pos):
        greet(barrier, a, p, 4)
    greet(barrier, "tp", core, 2)
    loads = [pltpu.make_async_copy(a, b, load_sem.at[k]) for k, (a, b) in enumerate(zip(ins, held))]
    order = [12, 16, 2, 3, 4, 6, 7, 8, 9, 0, 1, 5, 10, 11, 13, 15, 17, 14, 18, 19, 20]
    for k in order[:17]:
        loads[k].start()
    (uw_ref, un_ref, pw_ref, pn_ref, step_ref, forget_ref, inw_ref, inn_ref, ow_ref, on_ref,
     skip_ref, gate_ref, residual_ref, mgain_ref, outp_ref, fgain_ref, routes_ref, weights_ref,
     wg_ref, wu_ref, wd_ref) = held
    for k in order[:17]:
        loads[k].wait()
    for k in order[17:]:
        loads[k].start()

    swap = swap_matrix()
    earlier = (iota((64, 64), 0) < iota((64, 64), 1)).astype(BF16)
    expert = partner(iota((128, 64), 0))[1]
    named = [(expert == routes_ref[k : k + 1, :]).astype(F32) for k in range(2)]
    count = named[0] + named[1]
    rank = dot(count.astype(BF16), earlier)
    pick = [jnp.where(rank == r, count, 0.0).astype(BF16) for r in range(2)]
    for half in range(2):
        for r in range(2):
            slots[r] = dot(pick[r], residual_ref[:, half * 1024 : (half + 1) * 1024]).astype(BF16)

        def put_residual(at, block):
            res_out[at : at + 16, half] = block

        pack(lambda r, at, j: slots[r, at : at + 16, j * 128 : (j + 1) * 128], swap, put_residual, 128)
    pl.semaphore_wait(barrier, 10)
    greet(known_sem.at[0], "sp_2", pos[0], 4)

    for s, (p_ref, in_ref, o_ref, win, wout) in enumerate(
        ((pw_ref, inw_ref, ow_ref, win_w, wout_w), (pn_ref, inn_ref, on_ref, win_n, wout_n))
    ):
        n, first = SETS[s]
        tile_r = iota((n, 8 * n), 0)
        tile_c = iota((n, 8 * n), 1)
        tiler = (tile_r == lax.rem(tile_c, n)).astype(BF16)
        wr = iota((128, 8 * n), 0)
        wc = iota((128, 8 * n), 1)
        keep = (wr // 16) == (wc // n)
        for d in range(2):
            pr = p_ref[d, 0]
            pi = p_ref[d, 1]
            grow = jnp.exp(pr)
            lre = grow * jnp.cos(pi)
            lim = grow * jnp.sin(pi)
            nre = lre - 1.0
            step = jnp.sum(jnp.where(iota((16, 16), 0) == iota((16, 16), 1), step_ref[d, s : s + 1, :], 0.0), axis=1, keepdims=True)
            scale = step / (pr * pr + pi * pi)
            fre = (nre * pr + lim * pi) * scale
            fim = (lim * pr - nre * pi) * scale
            for ri, lam in ((0, lre), (1, lim)):
                parts = jnp.concatenate(split3(lam), axis=0)
                for h in range(2):
                    wide = dot(parts, tiler)
                    gr = lax.rem(iota((48, 8 * n), 0), 16)
                    gc = iota((48, 8 * n), 1) // n + 8 * h
                    row = jnp.sum(jnp.where(gr == gc, wide, 0.0), axis=0, keepdims=True)
                    lam_ref[2 * d + ri : 2 * d + ri + 1, first + 8 * n * h : first + 8 * n * (h + 1)] = row
            ere, eim = [], []
            for g in range(16):
                a = in_ref[d, 0, g * 16 : (g + 1) * 16, :]
                b = in_ref[d, 1, g * 16 : (g + 1) * 16, :]
                fr, fi = fre[g : g + 1], fim[g : g + 1]
                ere.append((fr * a - fi * b).astype(BF16))
                eim.append((fr * b + fi * a).astype(BF16))
            for h in range(2):
                for ri, rows in ((0, ere), (1, eim)):
                    part = jnp.concatenate(rows[8 * h : 8 * h + 8], axis=0)
                    win[d, ri, h] = jnp.where(keep, dot(part, tiler), 0.0).astype(BF16)
                    o = o_ref[d, ri, h * 128 : (h + 1) * 128, :]
                    o = (-o if ri else o).astype(BF16)
                    wout[d, ri, h] = jnp.where(keep, dot(o, tiler), 0.0).astype(BF16)

    pl.semaphore_wait(known_sem.at[0], 3)
    greet(known_sem.at[1], "sp_1", pos[1], 4)
    pr_ = iota((128, 128), 0)
    pc_ = iota((128, 128), 1)
    perm = (pc_ == lax.rem(pr_, 8) * 16 + pr_ // 8).astype(BF16)
    back = (pr_ == lax.rem(pc_, 8) * 16 + pc_ // 8).astype(BF16)
    u = [dot(perm, uw_ref[...]), dot(perm, un_ref[...])]
    ub = [x.astype(BF16) for x in u]
    for d in range(2):
        for s, win in enumerate((win_w, win_n)):
            n, first = SETS[s]
            for h in range(2):
                at = first + 8 * n * h
                for ri in range(2):
                    xs[d, ri, :, at : at + 8 * n] = dot(ub[s][:, h * 128 : (h + 1) * 128], win[d, ri, h])
    ef = jnp.concatenate(split3(jnp.exp(-forget_ref[...])), axis=0)
    ep = dot_nt(perm, ef).astype(BF16)
    sr = lax.rem(iota((192, NL), 0), 64)
    sc = iota((192, NL), 1)
    group_of = jnp.where(sc < 1024, sc // 64, 16 + (sc - 1024) // 32)
    for d in range(2):
        spread[d] = (sr == group_of + 32 * d).astype(BF16)
        es[d] = dot(ep, spread[d])

    def scan_step(i, state, c, keep_states):
        new = []
        for d in range(2):
            row = i if d == 0 else 15 - i
            at = pl.ds(pl.multiple_of(row * 8, 8), 8)
            lanes = slice(c * CHUNK, (c + 1) * CHUNK)
            lr = lam_ref[2 * d : 2 * d + 1, lanes]
            li = lam_ref[2 * d + 1 : 2 * d + 2, lanes]
            sre, sim = state[3 * d], state[3 * d + 1]
            e = es[d, at, lanes]
            nre = (lr * sre - li * sim) * e + xs[d, 0, at, lanes]
            nim = (lr * sim + li * sre) * e + xs[d, 1, at, lanes]
            if keep_states:
                xs[d, 0, at, lanes] = nre
                xs[d, 1, at, lanes] = nim
            new += [nre, nim, state[3 * d + 2] if keep_states else state[3 * d + 2] * e]
        return tuple(new)

    pl.semaphore_wait(known_sem.at[1], 3)
    greet(known_sem.at[2], "tp", core, 2)
    sub = iota((8, CHUNK), 0)
    ends = [[], []]
    for c in range(NL // CHUNK):
        zero = jnp.zeros((8, CHUNK), F32)
        one = jnp.ones((8, CHUNK), F32)
        state = lax.fori_loop(
            0, 16, lambda i, st: scan_step(i, st, c, False), (zero, zero, one, zero, zero, one)
        )
        lanes = slice(c * CHUNK, (c + 1) * CHUNK)
        for d in range(2):
            sre, sim, g = state[3 * d : 3 * d + 3]
            lr, li = lam_ref[2 * d : 2 * d + 1, lanes], lam_ref[2 * d + 1 : 2 * d + 2, lanes]
            for _ in range(4):
                lr, li = square(lr, li)
            place = sub if d == 0 else 7 - sub
            pre, pim = one, zero
            for k in (1, 2, 4):
                shift = k if d == 0 else 8 - k
                has = place >= k
                before_re = jnp.where(has, pltpu.roll(sre, shift, 0), 0.0) * g
                before_im = jnp.where(has, pltpu.roll(sim, shift, 0), 0.0) * g
                add_re, add_im = cmul(lr, li, before_re, before_im)
                sre, sim = sre + add_re, sim + add_im
                g = g * jnp.where(has, pltpu.roll(g, shift, 0), 1.0)
                tre, tim = cmul(lr, li, pre, pim)
                bit = lax.rem(place // k, 2) == 1
                pre, pim = jnp.where(bit, tre, pre), jnp.where(bit, tim, pim)
                lr, li = square(lr, li)
            edge = 7 if d == 0 else 0
            ends[d].append((sre[edge : edge + 1], sim[edge : edge + 1]))
            shift = 1 if d == 0 else 7
            has = place >= 1
            carry_ref[d, 0, :, lanes] = jnp.where(has, pltpu.roll(sre, shift, 0), 0.0)
            carry_ref[d, 1, :, lanes] = jnp.where(has, pltpu.roll(sim, shift, 0), 0.0)
            gx = jnp.where(has, pltpu.roll(g, shift, 0), 1.0)
            prod_ref[d, 0, :, lanes] = pre * gx
            prod_ref[d, 1, :, lanes] = pim * gx
            lam_ref[4 + 2 * d : 5 + 2 * d, lanes] = lr
            lam_ref[5 + 2 * d : 6 + 2 * d, lanes] = li

    fsum = lax.dot_general(
        jnp.ones((8, 128), F32), forget_ref[...], (((1,), (1,)), ((), ())),
        preferred_element_type=F32, precision=lax.Precision.HIGHEST,
    )[0:1]
    total = [
        [jnp.concatenate([e[q] for e in ends[d]], axis=1) for q in range(2)] for d in range(2)
    ]
    power = [[lam_ref[4 + 2 * d + q : 5 + 2 * d + q, :] for q in range(2)] for d in range(2)]
    enter = None
    pl.semaphore_wait(known_sem.at[2], 1)
    for stage, a in enumerate(axes):
        p = pos[stage]
        lines = [
            total[d][q][:, 384 * k : 384 * (k + 1)] for d in range(2) for q in range(2) for k in range(4)
        ]
        sums_sent = [x.astype(F32) for x in split3(fsum)] + [jnp.zeros((1, 64), F32)] * 13
        send[stage] = jnp.concatenate(
            [jnp.concatenate(lines, axis=0), jnp.concatenate(sums_sent, axis=0)], axis=1
        ).astype(BF16)
        copies = []
        for o in (1, 3, 2):
            there = lax.rem(p + o, 4)
            copies.append(
                pltpu.make_async_remote_copy(
                    src_ref=send.at[stage],
                    dst_ref=recv.at[stage, p],
                    send_sem=send_sem.at[stage, o],
                    recv_sem=recv_sem.at[stage, p],
                    device_id={a: there},
                    device_id_type=MESH,
                )
            )
            copies[-1].start()
        send_some(*BATCHES[stage], res_out, res_in, all_send.at[0], all_recv.at[0])
        for o in (1, 3, 2):
            there = lax.rem(p + o, 4)
            pltpu.make_async_remote_copy(
                src_ref=send.at[stage],
                dst_ref=recv.at[stage, there],
                send_sem=send_sem.at[stage, o],
                recv_sem=recv_sem.at[stage, there],
                device_id={a: there},
                device_id_type=MESH,
            ).wait_recv()
        recv[stage, p] = send[stage]
        came = [recv[stage, k].astype(F32) for k in range(4)]
        sums = jnp.concatenate(
            [jnp.sum(x[0:3, 384:448], axis=0, keepdims=True) for x in came], axis=0
        )
        parts = jnp.concatenate(split3(jnp.exp(-sums)), axis=1)
        for d in range(2):
            g = dot(parts, spread[d])
            lr, li = power[d]
            rre = rim = jnp.zeros((1, NL), F32)
            ire = iim = jnp.zeros((1, NL), F32)
            are, aim = jnp.ones((1, NL), F32), jnp.zeros((1, NL), F32)
            jre, jim = are, aim
            for step in range(4):
                k = step if d == 0 else 3 - step
                here = k == p
                ire, iim = jnp.where(here, rre, ire), jnp.where(here, rim, iim)
                nearer = (k < p) if d == 0 else (k > p)
                gr, gi = lr * g[k : k + 1], li * g[k : k + 1]
                tre, tim = (
                    jnp.concatenate([came[k][r : r + 1, 0:384] for r in range(at, at + 4)], axis=1)
                    for at in (8 * d, 8 * d + 4)
                )
                rre, rim = cmul(gr, gi, rre, rim)
                rre, rim = rre + tre, rim + tim
                nre, nim = cmul(gr, gi, jre, jim)
                jre, jim = jnp.where(nearer, nre, jre), jnp.where(nearer, nim, jim)
            total[d] = [rre, rim]
            lr, li = square(*square(lr, li))
            power[d] = [lr, li]
            if enter is None or len(enter) < 2:
                enter = (enter or []) + [[ire, iim, jre, jim]]
            else:
                bre, bim, cre, cim = enter[d]
                add_re, add_im = cmul(cre, cim, ire, iim)
                ncre, ncim = cmul(cre, cim, jre, jim)
                enter[d] = [bre + add_re, bim + add_im, ncre, ncim]
        fsum = jnp.sum(sums, axis=0, keepdims=True)
        for copy in copies:
            copy.wait_send()

    send_some(*BATCHES[3], res_out, res_in, all_send.at[0], all_recv.at[0])
    res_in[0] = res_out[0]
    for c in range(NL // CHUNK):
        lanes = slice(c * CHUNK, (c + 1) * CHUNK)
        state = []
        for d in range(2):
            cre, cim = enter[d][0][:, lanes], enter[d][1][:, lanes]
            add_re, add_im = cmul(prod_ref[d, 0, :, lanes], prod_ref[d, 1, :, lanes], cre, cim)
            state += [carry_ref[d, 0, :, lanes] + add_re, carry_ref[d, 1, :, lanes] + add_im, jnp.zeros((8, 128), F32)]
        lax.fori_loop(0, 16, lambda i, st: scan_step(i, st, c, True), tuple(state))

    for s, wout in enumerate((wout_w, wout_n)):
        n, first = SETS[s]
        for h in range(2):
            at = first + 8 * n * h
            y = None
            for d in range(2):
                for ri in range(2):
                    term = dot_nt(xs[d, ri, :, at : at + 8 * n].astype(BF16), wout[d, ri, h])
                    y = term if y is None else y + term
            ch = slice(h * 128, (h + 1) * 128)
            y = y + skip_ref[s : s + 1, ch].astype(F32) * u[s][:, ch]
            active = jax.nn.gelu(y, approximate=True)
            gr = iota((16, 128), 0)
            gc = iota((16, 128), 1)
            tiler = (gr == lax.rem(gc, 16)).astype(BF16)
            gate = dot(gate_ref[s, ch, :], tiler)
            gate = jnp.where(iota((128, 128), 0) // 16 == iota((128, 128), 1) // 16, gate, 0.0).astype(BF16)
            opened = jax.nn.sigmoid(dot(active.astype(BF16), gate))
            done = dot(back, (active * opened).astype(BF16)).astype(BF16)
            for half in range(2):
                mine[half, :, s * 256 + h * 128 : s * 256 + (h + 1) * 128] = done[half * 64 : (half + 1) * 64]

    copy = pltpu.make_async_remote_copy(
        src_ref=mine.at[1 - core],
        dst_ref=theirs,
        send_sem=tp_send,
        recv_sem=tp_recv,
        device_id={"tp": 1 - core},
        device_id_type=MESH,
    )
    copy.start()
    copy.wait()

    own, other = mine[core].astype(F32), theirs[...].astype(F32)
    low = jnp.where(core == 0, own, other)
    high = jnp.where(core == 0, other, own)
    joined = jnp.concatenate([low[:, :256], high[:, :256], low[:, 256:], high[:, 256:]], axis=1)
    scale = lax.rsqrt(jnp.mean(joined * joined, axis=1, keepdims=True) + epsilon)
    mixed = (joined * scale * mgain_ref[...]).astype(BF16)
    for r in range(2):
        slots[r] = dot(pick[r], mixed).astype(BF16)

    def put_mixed_out(at, block):
        mix_out[at : at + 16] = block

    pack(lambda r, at, j: slots[r, at : at + 16, j * 128 : (j + 1) * 128], swap, put_mixed_out, 128)
    for n, (first, last) in enumerate(PARTS):
        send_some(max(first, 1), last, mix_out, mix_in, all_send.at[1 + n], all_recv.at[1 + n])
    mix_in[0] = mix_out[0]

    loads[14].wait()
    for c in range(8):
        lanes = slice(c * 256, (c + 1) * 256)
        own_ref[:, lanes] = (
            residual_ref[:, lanes].astype(F32) + dot(mixed, outp_ref[:, lanes])
        ).astype(BF16)
    all_of(1, 128, res_out, res_in, all_send.at[0], all_recv.at[0]).wait_recv()
    for n, (first, last) in enumerate(PARTS):
        for half in range(2):

            def put_rows(r, at, j, rows):
                lanes = half * 1024 + j * 128
                rows_ref[n, r * 64 + at : r * 64 + at + 16, lanes : lanes + 128] = rows

            unpack(lambda at: res_in[first + at : first + at + 16, half], swap, put_rows, 64)

    eye = iota((64, 64), 0) == iota((64, 64), 1)
    def column(row):
        return jnp.sum(jnp.where(eye, row, 0.0), axis=1, keepdims=True)
    experts = partner(iota((64, 128), 1))[1].astype(F32)
    hits = [(column(routes_ref[k : k + 1, :].astype(F32)) == experts).astype(F32) for k in range(2)]
    w = [column(weights_ref[k : k + 1, :]) for k in range(2)]
    both = w[0] + w[1]
    before = (iota((64, 64), 1) < iota((64, 64), 0)).astype(BF16)
    ranks = dot(before, (hits[0] + hits[1]).astype(BF16))
    shares = hits[0] * (w[0] / both) + hits[1] * (w[1] / both)
    parts = []
    for r in range(2):
        share = jnp.where(ranks == r, shares, 0.0)
        first = share.astype(BF16)
        parts.append((first, (share - first.astype(F32)).astype(BF16)))

    for k in order[18:]:
        loads[k].wait()
    for n, (first, last) in enumerate(PARTS):
        all_of(max(first, 1), last, mix_out, mix_in, all_send.at[1 + n], all_recv.at[1 + n]).wait_recv()

        def put_mixed(r, at, j, rows):
            mixed_ref[r * 64 + at : r * 64 + at + 16, j * 128 : (j + 1) * 128] = rows

        unpack(lambda at: mix_in[first + at : first + at + 16], swap, put_mixed, 64)
        square_sum = jnp.zeros((128, 1), F32)
        for c in range(8):
            lanes = slice(c * 256, (c + 1) * 256)
            h = (rows_ref[n, :, lanes].astype(F32) + dot(mixed_ref[...], outp_ref[:, lanes])).astype(BF16)
            hidden_ref[:, lanes] = h
            wide = h.astype(F32)
            square_sum = square_sum + jnp.sum(wide * wide, axis=1, keepdims=True)
        scale = lax.rsqrt(square_sum / 2048.0 + epsilon)
        for c in range(8):
            lanes = slice(c * 256, (c + 1) * 256)
            normed_ref[:, lanes] = (hidden_ref[:, lanes].astype(F32) * scale * fgain_ref[:, lanes]).astype(BF16)

        def expert_step(lanes):
            g = dot(normed_ref[...], wg_ref[0, :, lanes])
            v = dot(normed_ref[...], wu_ref[0, :, lanes])
            inner_ref[:, lanes] = (jax.nn.silu(g) * v).astype(BF16)

        for c in range(5):
            expert_step(slice(c * 256, (c + 1) * 256))
        expert_step(slice(1280, 1408))

        for half in range(2):
            for c in range(4):
                lanes = slice(half * 1024 + c * 256, half * 1024 + (c + 1) * 256)
                y = dot(inner_ref[...], wd_ref[0, :, lanes]).astype(BF16)
                for r in range(2):
                    slots[r, 0:64, c * 256 : (c + 1) * 256] = y[r * 64 : (r + 1) * 64]

            def put_return(at, block):
                ret_out[half, first + at : first + at + 16] = block

            pack(lambda r, at, j: slots[r, at : at + 16, j * 128 : (j + 1) * 128], swap, put_return, 64)
            send_back(
                max(first, 1), last, ret_out.at[half], ret_in.at[half], all_send.at[3 + 2 * n + half],
                all_recv.at[3 + 2 * n + half],
            )
    for half in range(2):
        ret_in[half, 0] = ret_out[half, 0]

    y = [own_ref[:, c * 256 : (c + 1) * 256].astype(F32) for c in range(8)]
    for n, (first, last) in enumerate(PARTS):
        for half in range(2):
            all_of(
                max(first, 1), last, ret_out.at[half], ret_in.at[half], all_send.at[3 + 2 * n + half],
                all_recv.at[3 + 2 * n + half],
            ).wait_recv()

            def put_back(r, at, j, rows):
                back_ref[r, at : at + 16, j * 128 : (j + 1) * 128] = rows

            unpack(lambda at: ret_in[half, first + at : first + at + 16], swap, put_back, 64)
            for c in range(4):
                lanes = slice(c * 256, (c + 1) * 256)
                for r in range(2):
                    for part in parts[r]:
                        y[4 * half + c] = y[4 * half + c] + dot(part[:, first:last], back_ref[r, :, lanes])
    for c in range(8):
        out_ref[:, c * 256 : (c + 1) * 256] = y[c].astype(BF16)

    all_of(1, 128, res_out, res_in, all_send.at[0], all_recv.at[0]).wait_send()
    for n, (first, last) in enumerate(PARTS):
        first = max(first, 1)
        all_of(first, last, mix_out, mix_in, all_send.at[1 + n], all_recv.at[1 + n]).wait_send()
        for half in range(2):
            all_of(
                first, last, ret_out.at[half], ret_in.at[half], all_send.at[3 + 2 * n + half],
                all_recv.at[3 + 2 * n + half],
            ).wait_send()


def local(
    wide_inputs, narrow_inputs, wide_poles, narrow_poles, step_sizes, forget, wide_in_map,
    narrow_in_map, wide_out_map, narrow_out_map, skip_weight, gate_mix, residual, mixer_gain,
    out_proj, ffn_gain, routes, route_weights, gate_proj, up_proj, down_proj,
):
    ins = (
        wide_inputs, narrow_inputs, wide_poles, narrow_poles, step_sizes, forget.reshape(64, 128),
        wide_in_map.reshape(2, 2, 256, 64), narrow_in_map.reshape(2, 2, 256, 32),
        wide_out_map.reshape(2, 2, 256, 64), narrow_out_map.reshape(2, 2, 256, 32),
        skip_weight, gate_mix.reshape(2, 256, 16), residual, mixer_gain.reshape(1, 1024), out_proj,
        ffn_gain.reshape(1, 2048), routes.T, route_weights.T, gate_proj, up_proj, down_proj,
    )
    scratch = [pltpu.VMEM(a.shape, a.dtype) for a in ins]
    scratch += [
        pltpu.VMEM((2, 2, 2, 128, 512), BF16),
        pltpu.VMEM((2, 2, 2, 128, 256), BF16),
        pltpu.VMEM((2, 2, 2, 128, 512), BF16),
        pltpu.VMEM((2, 2, 2, 128, 256), BF16),
        pltpu.VMEM((2, 2, 128, NL), F32),
        pltpu.VMEM((2, 128, NL), F32),
        pltpu.VMEM((2, 192, NL), BF16),
        pltpu.VMEM((2, 2, 8, NL), F32),
        pltpu.VMEM((2, 2, 8, NL), F32),
        pltpu.VMEM((8, NL), F32),
        pltpu.VMEM((3, 16, 448), BF16),
        pltpu.VMEM((3, 4, 16, 448), BF16),
        pltpu.VMEM((2, 64, 512), BF16),
        pltpu.VMEM((64, 512), BF16),
        pltpu.VMEM((128, 2, 16, 128), BF16),
        pltpu.VMEM((128, 2, 16, 128), BF16),
        pltpu.VMEM((128, 16, 128), BF16),
        pltpu.VMEM((128, 16, 128), BF16),
        pltpu.VMEM((2, 128, 16, 128), BF16),
        pltpu.VMEM((2, 128, 16, 128), BF16),
        pltpu.VMEM((2, 128, 1024), BF16),
        pltpu.VMEM((2, 128, 2048), BF16),
        pltpu.VMEM((128, 1024), BF16),
        pltpu.VMEM((128, 2048), BF16),
        pltpu.VMEM((128, 2048), BF16),
        pltpu.VMEM((128, 1408), BF16),
        pltpu.VMEM((2, 64, 1024), BF16),
        pltpu.VMEM((64, 2048), BF16),
        pltpu.SemaphoreType.DMA((21,)),
        pltpu.SemaphoreType.DMA((3, 4)),
        pltpu.SemaphoreType.DMA((3, 4)),
        pltpu.SemaphoreType.DMA,
        pltpu.SemaphoreType.DMA,
        pltpu.SemaphoreType.DMA((7,)),
        pltpu.SemaphoreType.DMA((7,)),
        pltpu.SemaphoreType.REGULAR((3,)),
    ]
    return pl.pallas_call(
        layer_kernel,
        out_shape=jax.ShapeDtypeStruct((64, 2048), BF16),
        in_specs=[pl.BlockSpec(memory_space=pl.ANY)] * 21,
        out_specs=pl.BlockSpec(memory_space=pltpu.VMEM),
        scratch_shapes=scratch,
        compiler_params=pltpu.CompilerParams(
            collective_id=0, has_side_effects=True, vmem_limit_bytes=60 * 1024 * 1024
        ),
        name="layer",
    )(*ins)


def solution(mesh):
    finer = Mesh(mesh.devices.reshape(4, 4, 4, mesh.shape["tp"]), ("sp_0", "sp_1", "sp_2", "tp"))
    return jax.shard_map(
        local,
        mesh=finer,
        in_specs=(
            P(SP, "tp"),
            P(SP, "tp"),
            P(None, None, "tp", None),
            P(None, None, "tp", None),
            P(None, None, "tp"),
            P(None, None, "tp", SP),
            P(None, None, "tp", None, None),
            P(None, None, "tp", None, None),
            P(None, None, "tp", None, None),
            P(None, None, "tp", None, None),
            P(None, "tp"),
            P(None, "tp", None, None),
            P(SP_TP, None),
            P(),
            P(),
            P(),
            P(SP_TP, None),
            P(SP_TP, None),
            P(SP_TP, None, None),
            P(SP_TP, None, None),
            P(SP_TP, None, None),
        ),
        out_specs=P(SP_TP, None),
        check_vma=False,
    )
```

```python
import functools

import jax
import jax.numpy as jnp
from jax import lax
from jax.experimental import pallas as pl
from jax.experimental.pallas import tpu as pltpu
from jax.sharding import Mesh
from jax.sharding import PartitionSpec as P

SP = ("sp_0", "sp_1", "sp_2")
SP_TP = ("sp_0", "sp_1", "sp_2", "tp")
MESH = pl.DeviceIdType.MESH
epsilon = 1e-06
F32 = jnp.float32
BF16 = jnp.bfloat16
NL = 1536
SETS = ((64, 0), (32, 1024))
CHUNK = 512
BATCHES = ((97, 128), (65, 97), (33, 65), (1, 33))
PARTS = ((64, 128), (0, 64))


def dot(a, b):
    return lax.dot_general(a, b, (((1,), (0,)), ((), ())), preferred_element_type=F32)


def dot_nt(a, b):
    return lax.dot_general(a, b, (((1,), (1,)), ((), ())), preferred_element_type=F32)


def split3(x):
    first = x.astype(BF16)
    rest = x - first.astype(F32)
    second = rest.astype(BF16)
    third = (rest - second.astype(F32)).astype(BF16)
    return first, second, third


def iota(shape, dim):
    return lax.broadcasted_iota(jnp.int32, shape, dim)


def cmul(ar, ai, br, bi):
    return ar * br - ai * bi, ar * bi + ai * br


def square(ar, ai):
    return ar * ar - ai * ai, 2.0 * ar * ai


def scattered():
    steps = [(o // 32, o // 8 % 4, o // 2 % 4, o % 2) for o in range(128)]
    return [steps[o] for o in sorted(range(128), key=lambda o: (o > 0, o * 37 % 128))]


STEPS = scattered()
SIZES = (4, 4, 4, 2)


def send_some(first, last, out, arrived, send_sem, recv_sem, way=1):
    there = [
        [lax.rem(lax.axis_index(a) + n + way * s, n) for s in range(n)] for a, n in zip(SP_TP, SIZES)
    ]
    for o in reversed(range(max(first, 1), last)):
        pltpu.make_async_remote_copy(
            src_ref=out.at[o], dst_ref=arrived.at[o], send_sem=send_sem, recv_sem=recv_sem,
            device_id={a: there[k][STEPS[o][k]] for k, a in enumerate(SP_TP)}, device_id_type=MESH,
        ).start()


def all_of(first, last, out, arrived, send_sem, recv_sem):
    return pltpu.make_async_remote_copy(
        src_ref=out.at[pl.ds(first, last - first)], dst_ref=arrived.at[pl.ds(first, last - first)],
        send_sem=send_sem, recv_sem=recv_sem, device_id={"tp": 1 - lax.axis_index("tp")},
        device_id_type=MESH,
    )


def swap_matrix():
    r, c = iota((256, 256), 0), iota((256, 256), 1)
    return (lax.rem(r, 16) * 16 + r // 16 == c).astype(BF16)


def pack(rows, swap, put, blocks):
    for k in range(0, blocks, 32):
        both = jnp.concatenate(
            [
                jnp.concatenate([rows(q // 8, k + 16 * side, q % 8) for q in range(16)], axis=0)
                for side in range(2)
            ],
            axis=1,
        )
        done = dot(swap, both).astype(BF16)
        for side in range(2):
            put(k + 16 * side, done[:, side * 128 : (side + 1) * 128].reshape(16, 16, 128))


def unpack(block, swap, put, blocks):
    for k in range(0, blocks, 32):
        both = jnp.concatenate(
            [block(k + 16 * side).reshape(256, 128) for side in range(2)], axis=1
        )
        done = dot(swap, both).astype(BF16)
        for side in range(2):
            for q in range(16):
                put(q // 8, k + 16 * side, q % 8, done[q * 16 : (q + 1) * 16, side * 128 : (side + 1) * 128])


def layer_kernel(*refs):
    ins, out_ref, held = refs[:23], refs[23], refs[24 : 24 + 23]
    (win_w, win_n, wout_w, wout_n, xs, es, spread, carry_ref, prod_ref, lam_ref, send, recv, mine, theirs,
     res_out, res_in, mix_out, mix_in, ret_out, ret_in, slots, rows_ref, mixed_ref, hidden_ref, normed_ref, inner_ref,
     back_ref, own_ref,
     load_sem, send_sem, recv_sem, tp_send, tp_recv, all_send, all_recv, known_sem) = refs[47:]
    axes = ("sp_2", "sp_1", "sp_0")
    pos = [lax.axis_index(a) for a in axes]
    core = lax.axis_index("tp")

    barrier = pltpu.get_barrier_semaphore()

    def greet(semaphore, axis, place, size):
        for o in range(1, size):
            pl.semaphore_signal(semaphore, inc=1, device_id={axis: lax.rem(place + o, size)}, device_id_type=MESH)

    for a, p in zip(axes, pos):
        greet(barrier, a, p, 4)
    greet(barrier, "tp", core, 2)
    loads = [pltpu.make_async_copy(a, b, load_sem.at[k]) for k, (a, b) in enumerate(zip(ins, held))]
    order = [2, 3, 4, 6, 7, 0, 1, 5, 16, 12, 21, 22, 8, 9, 10, 11, 13, 15, 17, 14, 18, 19, 20]
    for k in order[:19]:
        loads[k].start()
    (uw_ref, un_ref, pw_ref, pn_ref, step_ref, forget_ref, inw_ref, inn_ref, ow_ref, on_ref,
     skip_ref, gate_ref, residual_ref, mgain_ref, outp_ref, fgain_ref, routes_ref, weights_ref,
     wg_ref, wu_ref, wd_ref, down_ref, across_ref) = held
    for k in order[:19]:
        loads[k].wait()
    for k in order[19:]:
        loads[k].start()

    swap = swap_matrix()
    earlier = (iota((64, 64), 0) < iota((64, 64), 1)).astype(BF16)
    def numbers(steps):
        there = [lax.rem(lax.axis_index(a) + t, n) for a, t, n in zip(SP_TP, steps, SIZES)]
        return ((there[0] * 4 + there[1]) * 4 + there[2]) * 2 + there[3]

    expert = numbers([down_ref[:, k : k + 1] for k in range(4)])
    named = [(expert == routes_ref[k : k + 1, :]).astype(F32) for k in range(2)]
    count = named[0] + named[1]
    rank = dot(count.astype(BF16), earlier)
    pick = [jnp.where(rank == r, count, 0.0).astype(BF16) for r in range(2)]
    pl.semaphore_wait(barrier, 10)
    greet(known_sem.at[0], "sp_2", pos[0], 4)

    def spreader(n):
        tiler = (iota((n, 8 * n), 0) == lax.rem(iota((n, 8 * n), 1), n)).astype(BF16)
        return tiler, iota((128, 8 * n), 0) // 16 == iota((128, 8 * n), 1) // n

    def build_out():
        for n, o_ref, wout in ((64, ow_ref, wout_w), (32, on_ref, wout_n)):
            tiler, keep = spreader(n)
            for d in range(2):
                for ri in range(2):
                    for h in range(2):
                        o = o_ref[d, ri, h * 128 : (h + 1) * 128, :]
                        o = (-o if ri else o).astype(BF16)
                        wout[d, ri, h] = jnp.where(keep, dot(o, tiler), 0.0).astype(BF16)

    for s, (p_ref, in_ref, o_ref, win, wout) in enumerate(
        ((pw_ref, inw_ref, ow_ref, win_w, wout_w), (pn_ref, inn_ref, on_ref, win_n, wout_n))
    ):
        n, first = SETS[s]
        tiler, keep = spreader(n)
        for d in range(2):
            pr = p_ref[d, 0]
            pi = p_ref[d, 1]
            grow = jnp.exp(pr)
            lre = grow * jnp.cos(pi)
            lim = grow * jnp.sin(pi)
            nre = lre - 1.0
            step = jnp.sum(jnp.where(iota((16, 16), 0) == iota((16, 16), 1), step_ref[d, s : s + 1, :], 0.0), axis=1, keepdims=True)
            scale = step / (pr * pr + pi * pi)
            fre = (nre * pr + lim * pi) * scale
            fim = (lim * pr - nre * pi) * scale
            for ri, lam in ((0, lre), (1, lim)):
                parts = jnp.concatenate(split3(lam), axis=0)
                for h in range(2):
                    wide = dot(parts, tiler)
                    gr = lax.rem(iota((48, 8 * n), 0), 16)
                    gc = iota((48, 8 * n), 1) // n + 8 * h
                    row = jnp.sum(jnp.where(gr == gc, wide, 0.0), axis=0, keepdims=True)
                    lam_ref[2 * d + ri : 2 * d + ri + 1, first + 8 * n * h : first + 8 * n * (h + 1)] = row
            ere, eim = [], []
            for g in range(16):
                a = in_ref[d, 0, g * 16 : (g + 1) * 16, :]
                b = in_ref[d, 1, g * 16 : (g + 1) * 16, :]
                fr, fi = fre[g : g + 1], fim[g : g + 1]
                ere.append((fr * a - fi * b).astype(BF16))
                eim.append((fr * b + fi * a).astype(BF16))
            for h in range(2):
                for ri, rows in ((0, ere), (1, eim)):
                    part = jnp.concatenate(rows[8 * h : 8 * h + 8], axis=0)
                    win[d, ri, h] = jnp.where(keep, dot(part, tiler), 0.0).astype(BF16)

    pl.semaphore_wait(known_sem.at[0], 3)
    greet(known_sem.at[1], "sp_1", pos[1], 4)
    pr_ = iota((128, 128), 0)
    pc_ = iota((128, 128), 1)
    perm = (pc_ == lax.rem(pr_, 8) * 16 + pr_ // 8).astype(BF16)
    back = (pr_ == lax.rem(pc_, 8) * 16 + pc_ // 8).astype(BF16)
    u = [dot(perm, uw_ref[...]), dot(perm, un_ref[...])]
    ub = [x.astype(BF16) for x in u]
    for d in range(2):
        for s, win in enumerate((win_w, win_n)):
            n, first = SETS[s]
            for h in range(2):
                at = first + 8 * n * h
                for ri in range(2):
                    xs[d, ri, :, at : at + 8 * n] = dot(ub[s][:, h * 128 : (h + 1) * 128], win[d, ri, h])
    ef = jnp.concatenate(split3(jnp.exp(-forget_ref[...])), axis=0)
    ep = dot_nt(perm, ef).astype(BF16)
    sr = lax.rem(iota((192, NL), 0), 64)
    sc = iota((192, NL), 1)
    group_of = jnp.where(sc < 1024, sc // 64, 16 + (sc - 1024) // 32)
    for d in range(2):
        spread[d] = (sr == group_of + 32 * d).astype(BF16)
        es[d] = dot(ep, spread[d])

    def scan_step(i, state, c, keep_states):
        new = []
        for d in range(2):
            row = i if d == 0 else 15 - i
            at = pl.ds(pl.multiple_of(row * 8, 8), 8)
            lanes = slice(c * CHUNK, (c + 1) * CHUNK)
            lr = lam_ref[2 * d : 2 * d + 1, lanes]
            li = lam_ref[2 * d + 1 : 2 * d + 2, lanes]
            sre, sim = state[3 * d], state[3 * d + 1]
            e = es[d, at, lanes]
            nre = (lr * sre - li * sim) * e + xs[d, 0, at, lanes]
            nim = (lr * sim + li * sre) * e + xs[d, 1, at, lanes]
            if keep_states:
                xs[d, 0, at, lanes] = nre
                xs[d, 1, at, lanes] = nim
            new += [nre, nim, state[3 * d + 2] if keep_states else state[3 * d + 2] * e]
        return tuple(new)

    pl.semaphore_wait(known_sem.at[1], 3)
    greet(known_sem.at[2], "tp", core, 2)
    sub = iota((8, CHUNK), 0)
    ends = [[], []]
    for c in range(NL // CHUNK):
        zero = jnp.zeros((8, CHUNK), F32)
        one = jnp.ones((8, CHUNK), F32)
        state = lax.fori_loop(
            0, 16, lambda i, st: scan_step(i, st, c, False), (zero, zero, one, zero, zero, one)
        )
        lanes = slice(c * CHUNK, (c + 1) * CHUNK)
        for d in range(2):
            sre, sim, g = state[3 * d : 3 * d + 3]
            lr, li = lam_ref[2 * d : 2 * d + 1, lanes], lam_ref[2 * d + 1 : 2 * d + 2, lanes]
            for _ in range(4):
                lr, li = square(lr, li)
            place = sub if d == 0 else 7 - sub
            pre, pim = one, zero
            for k in (1, 2, 4):
                shift = k if d == 0 else 8 - k
                has = place >= k
                before_re = jnp.where(has, pltpu.roll(sre, shift, 0), 0.0) * g
                before_im = jnp.where(has, pltpu.roll(sim, shift, 0), 0.0) * g
                add_re, add_im = cmul(lr, li, before_re, before_im)
                sre, sim = sre + add_re, sim + add_im
                g = g * jnp.where(has, pltpu.roll(g, shift, 0), 1.0)
                tre, tim = cmul(lr, li, pre, pim)
                bit = lax.rem(place // k, 2) == 1
                pre, pim = jnp.where(bit, tre, pre), jnp.where(bit, tim, pim)
                lr, li = square(lr, li)
            edge = 7 if d == 0 else 0
            ends[d].append((sre[edge : edge + 1], sim[edge : edge + 1]))
            shift = 1 if d == 0 else 7
            has = place >= 1
            carry_ref[d, 0, :, lanes] = jnp.where(has, pltpu.roll(sre, shift, 0), 0.0)
            carry_ref[d, 1, :, lanes] = jnp.where(has, pltpu.roll(sim, shift, 0), 0.0)
            gx = jnp.where(has, pltpu.roll(g, shift, 0), 1.0)
            prod_ref[d, 0, :, lanes] = pre * gx
            prod_ref[d, 1, :, lanes] = pim * gx
            lam_ref[4 + 2 * d : 5 + 2 * d, lanes] = lr
            lam_ref[5 + 2 * d : 6 + 2 * d, lanes] = li

    fsum = lax.dot_general(
        jnp.ones((8, 128), F32), forget_ref[...], (((1,), (1,)), ((), ())),
        preferred_element_type=F32, precision=lax.Precision.HIGHEST,
    )[0:1]
    total = [
        [jnp.concatenate([e[q] for e in ends[d]], axis=1) for q in range(2)] for d in range(2)
    ]
    power = [[lam_ref[4 + 2 * d + q : 5 + 2 * d + q, :] for q in range(2)] for d in range(2)]
    enter = None
    pl.semaphore_wait(known_sem.at[2], 1)
    for stage, a in enumerate(axes):
        p = pos[stage]
        lines = [
            total[d][q][:, 384 * k : 384 * (k + 1)] for d in range(2) for q in range(2) for k in range(4)
        ]
        sums_sent = [x.astype(F32) for x in split3(fsum)] + [jnp.zeros((1, 64), F32)] * 13
        send[stage] = jnp.concatenate(
            [jnp.concatenate(lines, axis=0), jnp.concatenate(sums_sent, axis=0)], axis=1
        ).astype(BF16)
        copies = []
        for o in (1, 3, 2):
            there = lax.rem(p + o, 4)
            copies.append(
                pltpu.make_async_remote_copy(
                    src_ref=send.at[stage],
                    dst_ref=recv.at[stage, p],
                    send_sem=send_sem.at[stage, o],
                    recv_sem=recv_sem.at[stage, p],
                    device_id={a: there},
                    device_id_type=MESH,
                )
            )
            copies[-1].start()
        if stage == 0:
            build_out()
            for half in range(2):
                for r in range(2):
                    slots[r] = dot(pick[r], residual_ref[:, half * 1024 : (half + 1) * 1024]).astype(BF16)

                def put_residual(at, block):
                    res_out[at : at + 16, half] = block

                pack(lambda r, at, j: slots[r, at : at + 16, j * 128 : (j + 1) * 128], swap, put_residual, 128)
        send_some(*BATCHES[stage], res_out, res_in, all_send.at[0], all_recv.at[0])
        for o in (1, 3, 2):
            there = lax.rem(p + o, 4)
            pltpu.make_async_remote_copy(
                src_ref=send.at[stage],
                dst_ref=recv.at[stage, there],
                send_sem=send_sem.at[stage, o],
                recv_sem=recv_sem.at[stage, there],
                device_id={a: there},
                device_id_type=MESH,
            ).wait_recv()
        recv[stage, p] = send[stage]
        came = [recv[stage, k].astype(F32) for k in range(4)]
        sums = jnp.concatenate(
            [jnp.sum(x[0:3, 384:448], axis=0, keepdims=True) for x in came], axis=0
        )
        parts = jnp.concatenate(split3(jnp.exp(-sums)), axis=1)
        for d in range(2):
            g = dot(parts, spread[d])
            lr, li = power[d]
            rre = rim = jnp.zeros((1, NL), F32)
            ire = iim = jnp.zeros((1, NL), F32)
            are, aim = jnp.ones((1, NL), F32), jnp.zeros((1, NL), F32)
            jre, jim = are, aim
            for step in range(4):
                k = step if d == 0 else 3 - step
                here = k == p
                ire, iim = jnp.where(here, rre, ire), jnp.where(here, rim, iim)
                nearer = (k < p) if d == 0 else (k > p)
                gr, gi = lr * g[k : k + 1], li * g[k : k + 1]
                tre, tim = (
                    jnp.concatenate([came[k][r : r + 1, 0:384] for r in range(at, at + 4)], axis=1)
                    for at in (8 * d, 8 * d + 4)
                )
                rre, rim = cmul(gr, gi, rre, rim)
                rre, rim = rre + tre, rim + tim
                nre, nim = cmul(gr, gi, jre, jim)
                jre, jim = jnp.where(nearer, nre, jre), jnp.where(nearer, nim, jim)
            total[d] = [rre, rim]
            lr, li = square(*square(lr, li))
            power[d] = [lr, li]
            if enter is None or len(enter) < 2:
                enter = (enter or []) + [[ire, iim, jre, jim]]
            else:
                bre, bim, cre, cim = enter[d]
                add_re, add_im = cmul(cre, cim, ire, iim)
                ncre, ncim = cmul(cre, cim, jre, jim)
                enter[d] = [bre + add_re, bim + add_im, ncre, ncim]
        fsum = jnp.sum(sums, axis=0, keepdims=True)
        for copy in copies:
            copy.wait_send()

    send_some(*BATCHES[3], res_out, res_in, all_send.at[0], all_recv.at[0])
    res_in[0] = res_out[0]
    for c in range(NL // CHUNK):
        lanes = slice(c * CHUNK, (c + 1) * CHUNK)
        state = []
        for d in range(2):
            cre, cim = enter[d][0][:, lanes], enter[d][1][:, lanes]
            add_re, add_im = cmul(prod_ref[d, 0, :, lanes], prod_ref[d, 1, :, lanes], cre, cim)
            state += [carry_ref[d, 0, :, lanes] + add_re, carry_ref[d, 1, :, lanes] + add_im, jnp.zeros((8, 128), F32)]
        lax.fori_loop(0, 16, lambda i, st: scan_step(i, st, c, True), tuple(state))

    for s, wout in enumerate((wout_w, wout_n)):
        n, first = SETS[s]
        for h in range(2):
            at = first + 8 * n * h
            y = None
            for d in range(2):
                for ri in range(2):
                    term = dot_nt(xs[d, ri, :, at : at + 8 * n].astype(BF16), wout[d, ri, h])
                    y = term if y is None else y + term
            ch = slice(h * 128, (h + 1) * 128)
            y = y + skip_ref[s : s + 1, ch].astype(F32) * u[s][:, ch]
            active = jax.nn.gelu(y, approximate=True)
            gr = iota((16, 128), 0)
            gc = iota((16, 128), 1)
            tiler = (gr == lax.rem(gc, 16)).astype(BF16)
            gate = dot(gate_ref[s, ch, :], tiler)
            gate = jnp.where(iota((128, 128), 0) // 16 == iota((128, 128), 1) // 16, gate, 0.0).astype(BF16)
            opened = jax.nn.sigmoid(dot(active.astype(BF16), gate))
            done = dot(back, (active * opened).astype(BF16)).astype(BF16)
            for half in range(2):
                mine[half, :, s * 256 + h * 128 : s * 256 + (h + 1) * 128] = done[half * 64 : (half + 1) * 64]

    copy = pltpu.make_async_remote_copy(
        src_ref=mine.at[1 - core],
        dst_ref=theirs,
        send_sem=tp_send,
        recv_sem=tp_recv,
        device_id={"tp": 1 - core},
        device_id_type=MESH,
    )
    copy.start()
    copy.wait()

    own, other = mine[core].astype(F32), theirs[...].astype(F32)
    low = jnp.where(core == 0, own, other)
    high = jnp.where(core == 0, other, own)
    joined = jnp.concatenate([low[:, :256], high[:, :256], low[:, 256:], high[:, 256:]], axis=1)
    scale = lax.rsqrt(jnp.mean(joined * joined, axis=1, keepdims=True) + epsilon)
    mixed = (joined * scale * mgain_ref[...]).astype(BF16)
    for r in range(2):
        slots[r] = dot(pick[r], mixed).astype(BF16)

    def put_mixed_out(at, block):
        mix_out[at : at + 16] = block

    pack(lambda r, at, j: slots[r, at : at + 16, j * 128 : (j + 1) * 128], swap, put_mixed_out, 128)
    for n, (first, last) in enumerate(PARTS):
        send_some(first, last, mix_out, mix_in, all_send.at[1 + n], all_recv.at[1 + n])
    mix_in[0] = mix_out[0]

    loads[14].wait()
    for c in range(8):
        lanes = slice(c * 256, (c + 1) * 256)
        own_ref[:, lanes] = (
            residual_ref[:, lanes].astype(F32) + dot(mixed, outp_ref[:, lanes])
        ).astype(BF16)
    all_of(1, 128, res_out, res_in, all_send.at[0], all_recv.at[0]).wait_recv()
    for n, (first, last) in enumerate(PARTS):
        for half in range(2):

            def put_rows(r, at, j, rows):
                lanes = half * 1024 + j * 128
                rows_ref[n, r * 64 + at : r * 64 + at + 16, lanes : lanes + 128] = rows

            unpack(lambda at: res_in[first + at : first + at + 16, half], swap, put_rows, 64)

    eye = iota((64, 64), 0) == iota((64, 64), 1)
    def column(row):
        return jnp.sum(jnp.where(eye, row, 0.0), axis=1, keepdims=True)
    experts = numbers([across_ref[k : k + 1, :] for k in range(4)]).astype(F32)
    hits = [(column(routes_ref[k : k + 1, :].astype(F32)) == experts).astype(F32) for k in range(2)]
    w = [column(weights_ref[k : k + 1, :]) for k in range(2)]
    both = w[0] + w[1]
    before = (iota((64, 64), 1) < iota((64, 64), 0)).astype(BF16)
    ranks = dot(before, (hits[0] + hits[1]).astype(BF16))
    shares = hits[0] * (w[0] / both) + hits[1] * (w[1] / both)
    parts = []
    for r in range(2):
        share = jnp.where(ranks == r, shares, 0.0)
        first = share.astype(BF16)
        parts.append((first, (share - first.astype(F32)).astype(BF16)))

    for k in order[20:]:
        loads[k].wait()
    for n, (first, last) in enumerate(PARTS):
        all_of(max(first, 1), last, mix_out, mix_in, all_send.at[1 + n], all_recv.at[1 + n]).wait_recv()

        def put_mixed(r, at, j, rows):
            mixed_ref[r * 64 + at : r * 64 + at + 16, j * 128 : (j + 1) * 128] = rows

        unpack(lambda at: mix_in[first + at : first + at + 16], swap, put_mixed, 64)
        square_sum = jnp.zeros((128, 1), F32)
        for c in range(8):
            lanes = slice(c * 256, (c + 1) * 256)
            h = (rows_ref[n, :, lanes].astype(F32) + dot(mixed_ref[...], outp_ref[:, lanes])).astype(BF16)
            hidden_ref[:, lanes] = h
            wide = h.astype(F32)
            square_sum = square_sum + jnp.sum(wide * wide, axis=1, keepdims=True)
        scale = lax.rsqrt(square_sum / 2048.0 + epsilon)
        for c in range(8):
            lanes = slice(c * 256, (c + 1) * 256)
            normed_ref[:, lanes] = (hidden_ref[:, lanes].astype(F32) * scale * fgain_ref[:, lanes]).astype(BF16)

        def expert_step(lanes):
            g = dot(normed_ref[...], wg_ref[0, :, lanes])
            v = dot(normed_ref[...], wu_ref[0, :, lanes])
            inner_ref[:, lanes] = (jax.nn.silu(g) * v).astype(BF16)

        for c in range(5):
            expert_step(slice(c * 256, (c + 1) * 256))
        expert_step(slice(1280, 1408))

        for half in range(2):
            for c in range(4):
                lanes = slice(half * 1024 + c * 256, half * 1024 + (c + 1) * 256)
                y = dot(inner_ref[...], wd_ref[0, :, lanes]).astype(BF16)
                for r in range(2):
                    slots[r, 0:64, c * 256 : (c + 1) * 256] = y[r * 64 : (r + 1) * 64]

            def put_return(at, block):
                ret_out[first + at : first + at + 16, half] = block

            pack(lambda r, at, j: slots[r, at : at + 16, j * 128 : (j + 1) * 128], swap, put_return, 64)
        send_some(first, last, ret_out, ret_in, all_send.at[3 + n], all_recv.at[3 + n], -1)
    ret_in[0] = ret_out[0]

    y = [own_ref[:, c * 256 : (c + 1) * 256].astype(F32) for c in range(8)]
    for n, (first, last) in enumerate(PARTS):
        all_of(max(first, 1), last, ret_out, ret_in, all_send.at[3 + n], all_recv.at[3 + n]).wait_recv()
        for half in range(2):

            def put_back(r, at, j, rows):
                back_ref[r, at : at + 16, j * 128 : (j + 1) * 128] = rows

            unpack(lambda at: ret_in[first + at : first + at + 16, half], swap, put_back, 64)
            for c in range(4):
                lanes = slice(c * 256, (c + 1) * 256)
                for r in range(2):
                    for part in parts[r]:
                        y[4 * half + c] = y[4 * half + c] + dot(part[:, first:last], back_ref[r, :, lanes])
    for c in range(8):
        out_ref[:, c * 256 : (c + 1) * 256] = y[c].astype(BF16)

    all_of(1, 128, res_out, res_in, all_send.at[0], all_recv.at[0]).wait_send()
    for n, (first, last) in enumerate(PARTS):
        first = max(first, 1)
        all_of(first, last, mix_out, mix_in, all_send.at[1 + n], all_recv.at[1 + n]).wait_send()
        all_of(first, last, ret_out, ret_in, all_send.at[3 + n], all_recv.at[3 + n]).wait_send()


def local(
    wide_inputs, narrow_inputs, wide_poles, narrow_poles, step_sizes, forget, wide_in_map,
    narrow_in_map, wide_out_map, narrow_out_map, skip_weight, gate_mix, residual, mixer_gain,
    out_proj, ffn_gain, routes, route_weights, gate_proj, up_proj, down_proj,
):
    ins = (
        wide_inputs, narrow_inputs, wide_poles, narrow_poles, step_sizes, forget.reshape(64, 128),
        wide_in_map.reshape(2, 2, 256, 64), narrow_in_map.reshape(2, 2, 256, 32),
        wide_out_map.reshape(2, 2, 256, 64), narrow_out_map.reshape(2, 2, 256, 32),
        skip_weight, gate_mix.reshape(2, 256, 16), residual, mixer_gain.reshape(1, 1024), out_proj,
        ffn_gain.reshape(1, 2048), routes.T, route_weights.T, gate_proj, up_proj, down_proj,
        jnp.asarray(STEPS, jnp.int32), jnp.asarray(STEPS, jnp.int32).T,
    )
    scratch = [pltpu.VMEM(a.shape, a.dtype) for a in ins]
    scratch += [
        pltpu.VMEM((2, 2, 2, 128, 512), BF16),
        pltpu.VMEM((2, 2, 2, 128, 256), BF16),
        pltpu.VMEM((2, 2, 2, 128, 512), BF16),
        pltpu.VMEM((2, 2, 2, 128, 256), BF16),
        pltpu.VMEM((2, 2, 128, NL), F32),
        pltpu.VMEM((2, 128, NL), F32),
        pltpu.VMEM((2, 192, NL), BF16),
        pltpu.VMEM((2, 2, 8, NL), F32),
        pltpu.VMEM((2, 2, 8, NL), F32),
        pltpu.VMEM((8, NL), F32),
        pltpu.VMEM((3, 16, 448), BF16),
        pltpu.VMEM((3, 4, 16, 448), BF16),
        pltpu.VMEM((2, 64, 512), BF16),
        pltpu.VMEM((64, 512), BF16),
        pltpu.VMEM((128, 2, 16, 128), BF16),
        pltpu.VMEM((128, 2, 16, 128), BF16),
        pltpu.VMEM((128, 16, 128), BF16),
        pltpu.VMEM((128, 16, 128), BF16),
        pltpu.VMEM((128, 2, 16, 128), BF16),
        pltpu.VMEM((128, 2, 16, 128), BF16),
        pltpu.VMEM((2, 128, 1024), BF16),
        pltpu.VMEM((2, 128, 2048), BF16),
        pltpu.VMEM((128, 1024), BF16),
        pltpu.VMEM((128, 2048), BF16),
        pltpu.VMEM((128, 2048), BF16),
        pltpu.VMEM((128, 1408), BF16),
        pltpu.VMEM((2, 64, 1024), BF16),
        pltpu.VMEM((64, 2048), BF16),
        pltpu.SemaphoreType.DMA((23,)),
        pltpu.SemaphoreType.DMA((3, 4)),
        pltpu.SemaphoreType.DMA((3, 4)),
        pltpu.SemaphoreType.DMA,
        pltpu.SemaphoreType.DMA,
        pltpu.SemaphoreType.DMA((7,)),
        pltpu.SemaphoreType.DMA((7,)),
        pltpu.SemaphoreType.REGULAR((3,)),
    ]
    return pl.pallas_call(
        layer_kernel,
        out_shape=jax.ShapeDtypeStruct((64, 2048), BF16),
        in_specs=[pl.BlockSpec(memory_space=pl.ANY)] * 23,
        out_specs=pl.BlockSpec(memory_space=pltpu.VMEM),
        scratch_shapes=scratch,
        compiler_params=pltpu.CompilerParams(
            collective_id=0, has_side_effects=True, vmem_limit_bytes=60 * 1024 * 1024
        ),
        name="layer",
    )(*ins)


def solution(mesh):
    finer = Mesh(mesh.devices.reshape(4, 4, 4, mesh.shape["tp"]), ("sp_0", "sp_1", "sp_2", "tp"))
    return jax.shard_map(
        local,
        mesh=finer,
        in_specs=(
            P(SP, "tp"),
            P(SP, "tp"),
            P(None, None, "tp", None),
            P(None, None, "tp", None),
            P(None, None, "tp"),
            P(None, None, "tp", SP),
            P(None, None, "tp", None, None),
            P(None, None, "tp", None, None),
            P(None, None, "tp", None, None),
            P(None, None, "tp", None, None),
            P(None, "tp"),
            P(None, "tp", None, None),
            P(SP_TP, None),
            P(),
            P(),
            P(),
            P(SP_TP, None),
            P(SP_TP, None),
            P(SP_TP, None, None),
            P(SP_TP, None, None),
            P(SP_TP, None, None),
        ),
        out_specs=P(SP_TP, None),
        check_vma=False,
    )
```

```python
import functools

import jax
import jax.numpy as jnp
from jax import lax
from jax.experimental import pallas as pl
from jax.experimental.pallas import tpu as pltpu
from jax.sharding import Mesh
from jax.sharding import PartitionSpec as P

SP = ("sp_0", "sp_1", "sp_2")
SP_TP = ("sp_0", "sp_1", "sp_2", "tp")
MESH = pl.DeviceIdType.MESH
epsilon = 1e-06
F32 = jnp.float32
BF16 = jnp.bfloat16
NL = 1536
SETS = ((64, 0), (32, 1024))
CHUNK = 512
BATCHES = ((108, 128), (86, 108), (62, 86), (1, 62))
PARTS = ((64, 128), (0, 64))


def dot(a, b):
    return lax.dot_general(a, b, (((1,), (0,)), ((), ())), preferred_element_type=F32)


def dot_nt(a, b):
    return lax.dot_general(a, b, (((1,), (1,)), ((), ())), preferred_element_type=F32)


def split3(x):
    first = x.astype(BF16)
    rest = x - first.astype(F32)
    second = rest.astype(BF16)
    third = (rest - second.astype(F32)).astype(BF16)
    return first, second, third


def iota(shape, dim):
    return lax.broadcasted_iota(jnp.int32, shape, dim)


def cmul(ar, ai, br, bi):
    return ar * br - ai * bi, ar * bi + ai * br


def square(ar, ai):
    return ar * ar - ai * ai, 2.0 * ar * ai


def scattered():
    steps = [(o // 32, o // 8 % 4, o // 2 % 4, o % 2) for o in range(128)]
    return [steps[o] for o in sorted(range(128), key=lambda o: (o > 0, o * 37 % 128))]


STEPS = scattered()
SIZES = (4, 4, 4, 2)


def send_some(first, last, out, arrived, send_sem, recv_sem, way=1):
    there = [
        [lax.rem(lax.axis_index(a) + n + way * s, n) for s in range(n)] for a, n in zip(SP_TP, SIZES)
    ]
    for o in reversed(range(max(first, 1), last)):
        pltpu.make_async_remote_copy(
            src_ref=out.at[o], dst_ref=arrived.at[o], send_sem=send_sem, recv_sem=recv_sem,
            device_id={a: there[k][STEPS[o][k]] for k, a in enumerate(SP_TP)}, device_id_type=MESH,
        ).start()


def all_of(first, last, out, arrived, send_sem, recv_sem):
    return pltpu.make_async_remote_copy(
        src_ref=out.at[pl.ds(first, last - first)], dst_ref=arrived.at[pl.ds(first, last - first)],
        send_sem=send_sem, recv_sem=recv_sem, device_id={"tp": 1 - lax.axis_index("tp")},
        device_id_type=MESH,
    )


def swap_matrix():
    r, c = iota((256, 256), 0), iota((256, 256), 1)
    return (lax.rem(r, 16) * 16 + r // 16 == c).astype(BF16)


def pack(rows, swap, put, blocks):
    for k in range(0, blocks, 32):
        both = jnp.concatenate(
            [
                jnp.concatenate([rows(q // 8, k + 16 * side, q % 8) for q in range(16)], axis=0)
                for side in range(2)
            ],
            axis=1,
        )
        done = dot(swap, both).astype(BF16)
        for side in range(2):
            put(k + 16 * side, done[:, side * 128 : (side + 1) * 128].reshape(16, 16, 128))


def unpack(block, swap, put, blocks):
    for k in range(0, blocks, 32):
        both = jnp.concatenate(
            [block(k + 16 * side).reshape(256, 128) for side in range(2)], axis=1
        )
        done = dot(swap, both).astype(BF16)
        for side in range(2):
            for q in range(16):
                put(q // 8, k + 16 * side, q % 8, done[q * 16 : (q + 1) * 16, side * 128 : (side + 1) * 128])


def layer_kernel(*refs):
    ins, out_ref, held = refs[:23], refs[23], refs[24 : 24 + 23]
    (win_w, win_n, wout_w, wout_n, xs, es, spread, carry_ref, prod_ref, lam_ref, send, recv, mine, theirs,
     res_out, res_in, mix_out, mix_in, ret_out, ret_in, slots, rows_ref, mixed_ref, hidden_ref, normed_ref, inner_ref,
     back_ref, own_ref,
     load_sem, send_sem, recv_sem, tp_send, tp_recv, all_send, all_recv, known_sem) = refs[47:]
    axes = ("sp_2", "sp_1", "sp_0")
    pos = [lax.axis_index(a) for a in axes]
    core = lax.axis_index("tp")

    barrier = pltpu.get_barrier_semaphore()

    def greet(semaphore, axis, place, size):
        for o in range(1, size):
            pl.semaphore_signal(semaphore, inc=1, device_id={axis: lax.rem(place + o, size)}, device_id_type=MESH)

    for a, p in zip(axes, pos):
        greet(barrier, a, p, 4)
    greet(barrier, "tp", core, 2)
    loads = [pltpu.make_async_copy(a, b, load_sem.at[k]) for k, (a, b) in enumerate(zip(ins, held))]
    order = [2, 3, 4, 6, 7, 0, 1, 5, 16, 12, 21, 22, 8, 9, 10, 11, 13, 15, 17, 14, 18, 19, 20]
    for k in order[:19]:
        loads[k].start()
    (uw_ref, un_ref, pw_ref, pn_ref, step_ref, forget_ref, inw_ref, inn_ref, ow_ref, on_ref,
     skip_ref, gate_ref, residual_ref, mgain_ref, outp_ref, fgain_ref, routes_ref, weights_ref,
     wg_ref, wu_ref, wd_ref, down_ref, across_ref) = held
    for k in order[:8]:
        loads[k].wait()

    def spreader(n):
        tiler = (iota((n, 8 * n), 0) == lax.rem(iota((n, 8 * n), 1), n)).astype(BF16)
        return tiler, iota((128, 8 * n), 0) // 16 == iota((128, 8 * n), 1) // n

    def build_out():
        for n, o_ref, wout in ((64, ow_ref, wout_w), (32, on_ref, wout_n)):
            tiler, keep = spreader(n)
            for d in range(2):
                for ri in range(2):
                    for h in range(2):
                        o = o_ref[d, ri, h * 128 : (h + 1) * 128, :]
                        o = (-o if ri else o).astype(BF16)
                        wout[d, ri, h] = jnp.where(keep, dot(o, tiler), 0.0).astype(BF16)

    for s, (p_ref, in_ref, o_ref, win, wout) in enumerate(
        ((pw_ref, inw_ref, ow_ref, win_w, wout_w), (pn_ref, inn_ref, on_ref, win_n, wout_n))
    ):
        n, first = SETS[s]
        tiler, keep = spreader(n)
        for d in range(2):
            pr = p_ref[d, 0]
            pi = p_ref[d, 1]
            grow = jnp.exp(pr)
            lre = grow * jnp.cos(pi)
            lim = grow * jnp.sin(pi)
            nre = lre - 1.0
            step = jnp.sum(jnp.where(iota((16, 16), 0) == iota((16, 16), 1), step_ref[d, s : s + 1, :], 0.0), axis=1, keepdims=True)
            scale = step / (pr * pr + pi * pi)
            fre = (nre * pr + lim * pi) * scale
            fim = (lim * pr - nre * pi) * scale
            for ri, lam in ((0, lre), (1, lim)):
                parts = jnp.concatenate(split3(lam), axis=0)
                for h in range(2):
                    wide = dot(parts, tiler)
                    gr = lax.rem(iota((48, 8 * n), 0), 16)
                    gc = iota((48, 8 * n), 1) // n + 8 * h
                    row = jnp.sum(jnp.where(gr == gc, wide, 0.0), axis=0, keepdims=True)
                    lam_ref[2 * d + ri : 2 * d + ri + 1, first + 8 * n * h : first + 8 * n * (h + 1)] = row
            ere, eim = [], []
            for g in range(16):
                a = in_ref[d, 0, g * 16 : (g + 1) * 16, :]
                b = in_ref[d, 1, g * 16 : (g + 1) * 16, :]
                fr, fi = fre[g : g + 1], fim[g : g + 1]
                ere.append((fr * a - fi * b).astype(BF16))
                eim.append((fr * b + fi * a).astype(BF16))
            for h in range(2):
                for ri, rows in ((0, ere), (1, eim)):
                    part = jnp.concatenate(rows[8 * h : 8 * h + 8], axis=0)
                    win[d, ri, h] = jnp.where(keep, dot(part, tiler), 0.0).astype(BF16)

    for k in order[8:19]:
        loads[k].wait()
    for k in order[19:]:
        loads[k].start()
    pl.semaphore_wait(barrier, 10)
    greet(known_sem.at[0], "sp_2", pos[0], 4)
    pr_ = iota((128, 128), 0)
    pc_ = iota((128, 128), 1)
    perm = (pc_ == lax.rem(pr_, 8) * 16 + pr_ // 8).astype(BF16)
    back = (pr_ == lax.rem(pc_, 8) * 16 + pc_ // 8).astype(BF16)
    u = [dot(perm, uw_ref[...]), dot(perm, un_ref[...])]
    ub = [x.astype(BF16) for x in u]
    for d in range(2):
        for s, win in enumerate((win_w, win_n)):
            n, first = SETS[s]
            for h in range(2):
                at = first + 8 * n * h
                for ri in range(2):
                    xs[d, ri, :, at : at + 8 * n] = dot(ub[s][:, h * 128 : (h + 1) * 128], win[d, ri, h])
    ef = jnp.concatenate(split3(jnp.exp(-forget_ref[...])), axis=0)
    ep = dot_nt(perm, ef).astype(BF16)
    sr = lax.rem(iota((192, NL), 0), 64)
    sc = iota((192, NL), 1)
    group_of = jnp.where(sc < 1024, sc // 64, 16 + (sc - 1024) // 32)
    for d in range(2):
        spread[d] = (sr == group_of + 32 * d).astype(BF16)
        es[d] = dot(ep, spread[d])

    def scan_step(i, state, c, keep_states):
        new = []
        for d in range(2):
            row = i if d == 0 else 15 - i
            at = pl.ds(pl.multiple_of(row * 8, 8), 8)
            lanes = slice(c * CHUNK, (c + 1) * CHUNK)
            lr = lam_ref[2 * d : 2 * d + 1, lanes]
            li = lam_ref[2 * d + 1 : 2 * d + 2, lanes]
            sre, sim = state[3 * d], state[3 * d + 1]
            e = es[d, at, lanes]
            nre = (lr * sre - li * sim) * e + xs[d, 0, at, lanes]
            nim = (lr * sim + li * sre) * e + xs[d, 1, at, lanes]
            if keep_states:
                xs[d, 0, at, lanes] = nre
                xs[d, 1, at, lanes] = nim
            new += [nre, nim, state[3 * d + 2] if keep_states else state[3 * d + 2] * e]
        return tuple(new)

    sub = iota((8, CHUNK), 0)
    ends = [[], []]
    for c in range(NL // CHUNK):
        zero = jnp.zeros((8, CHUNK), F32)
        one = jnp.ones((8, CHUNK), F32)
        state = lax.fori_loop(
            0, 16, lambda i, st: scan_step(i, st, c, False), (zero, zero, one, zero, zero, one)
        )
        lanes = slice(c * CHUNK, (c + 1) * CHUNK)
        for d in range(2):
            sre, sim, g = state[3 * d : 3 * d + 3]
            lr, li = lam_ref[2 * d : 2 * d + 1, lanes], lam_ref[2 * d + 1 : 2 * d + 2, lanes]
            for _ in range(4):
                lr, li = square(lr, li)
            place = sub if d == 0 else 7 - sub
            pre, pim = one, zero
            for k in (1, 2, 4):
                shift = k if d == 0 else 8 - k
                has = place >= k
                before_re = jnp.where(has, pltpu.roll(sre, shift, 0), 0.0) * g
                before_im = jnp.where(has, pltpu.roll(sim, shift, 0), 0.0) * g
                add_re, add_im = cmul(lr, li, before_re, before_im)
                sre, sim = sre + add_re, sim + add_im
                g = g * jnp.where(has, pltpu.roll(g, shift, 0), 1.0)
                tre, tim = cmul(lr, li, pre, pim)
                bit = lax.rem(place // k, 2) == 1
                pre, pim = jnp.where(bit, tre, pre), jnp.where(bit, tim, pim)
                lr, li = square(lr, li)
            edge = 7 if d == 0 else 0
            ends[d].append((sre[edge : edge + 1], sim[edge : edge + 1]))
            shift = 1 if d == 0 else 7
            has = place >= 1
            carry_ref[d, 0, :, lanes] = jnp.where(has, pltpu.roll(sre, shift, 0), 0.0)
            carry_ref[d, 1, :, lanes] = jnp.where(has, pltpu.roll(sim, shift, 0), 0.0)
            gx = jnp.where(has, pltpu.roll(g, shift, 0), 1.0)
            prod_ref[d, 0, :, lanes] = pre * gx
            prod_ref[d, 1, :, lanes] = pim * gx
            lam_ref[4 + 2 * d : 5 + 2 * d, lanes] = lr
            lam_ref[5 + 2 * d : 6 + 2 * d, lanes] = li

    fsum = lax.dot_general(
        jnp.ones((8, 128), F32), forget_ref[...], (((1,), (1,)), ((), ())),
        preferred_element_type=F32, precision=lax.Precision.HIGHEST,
    )[0:1]
    total = [
        [jnp.concatenate([e[q] for e in ends[d]], axis=1) for q in range(2)] for d in range(2)
    ]
    power = [[lam_ref[4 + 2 * d + q : 5 + 2 * d + q, :] for q in range(2)] for d in range(2)]
    enter = None
    pl.semaphore_wait(known_sem.at[0], 3)
    greet(known_sem.at[1], "sp_1", pos[1], 4)
    for stage, a in enumerate(axes):
        p = pos[stage]
        lines = [
            total[d][q][:, 384 * k : 384 * (k + 1)] for d in range(2) for q in range(2) for k in range(4)
        ]
        sums_sent = [x.astype(F32) for x in split3(fsum)] + [jnp.zeros((1, 64), F32)] * 13
        send[stage] = jnp.concatenate(
            [jnp.concatenate(lines, axis=0), jnp.concatenate(sums_sent, axis=0)], axis=1
        ).astype(BF16)
        copies = []
        for o in (1, 3, 2):
            there = lax.rem(p + o, 4)
            copies.append(
                pltpu.make_async_remote_copy(
                    src_ref=send.at[stage],
                    dst_ref=recv.at[stage, p],
                    send_sem=send_sem.at[stage, o],
                    recv_sem=recv_sem.at[stage, p],
                    device_id={a: there},
                    device_id_type=MESH,
                )
            )
            copies[-1].start()
        if stage == 0:
            build_out()
            swap = swap_matrix()
            earlier = (iota((64, 64), 0) < iota((64, 64), 1)).astype(BF16)
            def numbers(steps):
                there = [lax.rem(lax.axis_index(a) + t, n) for a, t, n in zip(SP_TP, steps, SIZES)]
                return ((there[0] * 4 + there[1]) * 4 + there[2]) * 2 + there[3]

            expert = numbers([down_ref[:, k : k + 1] for k in range(4)])
            named = [(expert == routes_ref[k : k + 1, :]).astype(F32) for k in range(2)]
            count = named[0] + named[1]
            rank = dot(count.astype(BF16), earlier)
            pick = [jnp.where(rank == r, count, 0.0).astype(BF16) for r in range(2)]
            for half in range(2):
                for r in range(2):
                    slots[r] = dot(pick[r], residual_ref[:, half * 1024 : (half + 1) * 1024]).astype(BF16)

                def put_residual(at, block):
                    res_out[at : at + 16, half] = block

                pack(lambda r, at, j: slots[r, at : at + 16, j * 128 : (j + 1) * 128], swap, put_residual, 128)
            pl.semaphore_wait(known_sem.at[1], 3)
            greet(known_sem.at[2], "tp", core, 2)
            pl.semaphore_wait(known_sem.at[2], 1)
        send_some(*BATCHES[stage], res_out, res_in, all_send.at[0], all_recv.at[0])
        for o in (1, 3, 2):
            there = lax.rem(p + o, 4)
            pltpu.make_async_remote_copy(
                src_ref=send.at[stage],
                dst_ref=recv.at[stage, there],
                send_sem=send_sem.at[stage, o],
                recv_sem=recv_sem.at[stage, there],
                device_id={a: there},
                device_id_type=MESH,
            ).wait_recv()
        recv[stage, p] = send[stage]
        came = [recv[stage, k].astype(F32) for k in range(4)]
        sums = jnp.concatenate(
            [jnp.sum(x[0:3, 384:448], axis=0, keepdims=True) for x in came], axis=0
        )
        parts = jnp.concatenate(split3(jnp.exp(-sums)), axis=1)
        for d in range(2):
            g = dot(parts, spread[d])
            lr, li = power[d]
            rre = rim = jnp.zeros((1, NL), F32)
            ire = iim = jnp.zeros((1, NL), F32)
            are, aim = jnp.ones((1, NL), F32), jnp.zeros((1, NL), F32)
            jre, jim = are, aim
            for step in range(4):
                k = step if d == 0 else 3 - step
                here = k == p
                ire, iim = jnp.where(here, rre, ire), jnp.where(here, rim, iim)
                nearer = (k < p) if d == 0 else (k > p)
                gr, gi = lr * g[k : k + 1], li * g[k : k + 1]
                tre, tim = (
                    jnp.concatenate([came[k][r : r + 1, 0:384] for r in range(at, at + 4)], axis=1)
                    for at in (8 * d, 8 * d + 4)
                )
                rre, rim = cmul(gr, gi, rre, rim)
                rre, rim = rre + tre, rim + tim
                nre, nim = cmul(gr, gi, jre, jim)
                jre, jim = jnp.where(nearer, nre, jre), jnp.where(nearer, nim, jim)
            total[d] = [rre, rim]
            lr, li = square(*square(lr, li))
            power[d] = [lr, li]
            if enter is None or len(enter) < 2:
                enter = (enter or []) + [[ire, iim, jre, jim]]
            else:
                bre, bim, cre, cim = enter[d]
                add_re, add_im = cmul(cre, cim, ire, iim)
                ncre, ncim = cmul(cre, cim, jre, jim)
                enter[d] = [bre + add_re, bim + add_im, ncre, ncim]
        fsum = jnp.sum(sums, axis=0, keepdims=True)
        for copy in copies:
            copy.wait_send()

    send_some(*BATCHES[3], res_out, res_in, all_send.at[0], all_recv.at[0])
    res_in[0] = res_out[0]
    for c in range(NL // CHUNK):
        lanes = slice(c * CHUNK, (c + 1) * CHUNK)
        state = []
        for d in range(2):
            cre, cim = enter[d][0][:, lanes], enter[d][1][:, lanes]
            add_re, add_im = cmul(prod_ref[d, 0, :, lanes], prod_ref[d, 1, :, lanes], cre, cim)
            state += [carry_ref[d, 0, :, lanes] + add_re, carry_ref[d, 1, :, lanes] + add_im, jnp.zeros((8, 128), F32)]
        lax.fori_loop(0, 16, lambda i, st: scan_step(i, st, c, True), tuple(state))

    for s, wout in enumerate((wout_w, wout_n)):
        n, first = SETS[s]
        for h in range(2):
            at = first + 8 * n * h
            y = None
            for d in range(2):
                for ri in range(2):
                    term = dot_nt(xs[d, ri, :, at : at + 8 * n].astype(BF16), wout[d, ri, h])
                    y = term if y is None else y + term
            ch = slice(h * 128, (h + 1) * 128)
            y = y + skip_ref[s : s + 1, ch].astype(F32) * u[s][:, ch]
            active = jax.nn.gelu(y, approximate=True)
            gr = iota((16, 128), 0)
            gc = iota((16, 128), 1)
            tiler = (gr == lax.rem(gc, 16)).astype(BF16)
            gate = dot(gate_ref[s, ch, :], tiler)
            gate = jnp.where(iota((128, 128), 0) // 16 == iota((128, 128), 1) // 16, gate, 0.0).astype(BF16)
            opened = jax.nn.sigmoid(dot(active.astype(BF16), gate))
            done = dot(back, (active * opened).astype(BF16)).astype(BF16)
            for half in range(2):
                mine[half, :, s * 256 + h * 128 : s * 256 + (h + 1) * 128] = done[half * 64 : (half + 1) * 64]

    copy = pltpu.make_async_remote_copy(
        src_ref=mine.at[1 - core],
        dst_ref=theirs,
        send_sem=tp_send,
        recv_sem=tp_recv,
        device_id={"tp": 1 - core},
        device_id_type=MESH,
    )
    copy.start()
    copy.wait()

    own, other = mine[core].astype(F32), theirs[...].astype(F32)
    low = jnp.where(core == 0, own, other)
    high = jnp.where(core == 0, other, own)
    joined = jnp.concatenate([low[:, :256], high[:, :256], low[:, 256:], high[:, 256:]], axis=1)
    scale = lax.rsqrt(jnp.mean(joined * joined, axis=1, keepdims=True) + epsilon)
    mixed = (joined * scale * mgain_ref[...]).astype(BF16)
    for n, (first, last) in enumerate(PARTS):
        for r in range(2):
            slots[r, 0:64] = dot(pick[r][first:last], mixed).astype(BF16)

        def put_mixed_out(at, block):
            mix_out[first + at : first + at + 16] = block

        pack(lambda r, at, j: slots[r, at : at + 16, j * 128 : (j + 1) * 128], swap, put_mixed_out, 64)
        send_some(first, last, mix_out, mix_in, all_send.at[1 + n], all_recv.at[1 + n])
    mix_in[0] = mix_out[0]

    loads[14].wait()
    for c in range(8):
        lanes = slice(c * 256, (c + 1) * 256)
        own_ref[:, lanes] = (
            residual_ref[:, lanes].astype(F32) + dot(mixed, outp_ref[:, lanes])
        ).astype(BF16)
    all_of(1, 128, res_out, res_in, all_send.at[0], all_recv.at[0]).wait_recv()
    for n, (first, last) in enumerate(PARTS):
        for half in range(2):

            def put_rows(r, at, j, rows):
                lanes = half * 1024 + j * 128
                rows_ref[n, r * 64 + at : r * 64 + at + 16, lanes : lanes + 128] = rows

            unpack(lambda at: res_in[first + at : first + at + 16, half], swap, put_rows, 64)

    eye = iota((64, 64), 0) == iota((64, 64), 1)
    def column(row):
        return jnp.sum(jnp.where(eye, row, 0.0), axis=1, keepdims=True)
    experts = numbers([across_ref[k : k + 1, :] for k in range(4)]).astype(F32)
    hits = [(column(routes_ref[k : k + 1, :].astype(F32)) == experts).astype(F32) for k in range(2)]
    w = [column(weights_ref[k : k + 1, :]) for k in range(2)]
    both = w[0] + w[1]
    before = (iota((64, 64), 1) < iota((64, 64), 0)).astype(BF16)
    ranks = dot(before, (hits[0] + hits[1]).astype(BF16))
    shares = hits[0] * (w[0] / both) + hits[1] * (w[1] / both)
    parts = []
    for r in range(2):
        share = jnp.where(ranks == r, shares, 0.0)
        first = share.astype(BF16)
        parts.append((first, (share - first.astype(F32)).astype(BF16)))

    for k in order[20:]:
        loads[k].wait()
    for n, (first, last) in enumerate(PARTS):
        all_of(max(first, 1), last, mix_out, mix_in, all_send.at[1 + n], all_recv.at[1 + n]).wait_recv()

        def put_mixed(r, at, j, rows):
            mixed_ref[r * 64 + at : r * 64 + at + 16, j * 128 : (j + 1) * 128] = rows

        unpack(lambda at: mix_in[first + at : first + at + 16], swap, put_mixed, 64)
        square_sum = jnp.zeros((128, 1), F32)
        for c in range(8):
            lanes = slice(c * 256, (c + 1) * 256)
            h = (rows_ref[n, :, lanes].astype(F32) + dot(mixed_ref[...], outp_ref[:, lanes])).astype(BF16)
            hidden_ref[:, lanes] = h
            wide = h.astype(F32)
            square_sum = square_sum + jnp.sum(wide * wide, axis=1, keepdims=True)
        scale = lax.rsqrt(square_sum / 2048.0 + epsilon)
        for c in range(8):
            lanes = slice(c * 256, (c + 1) * 256)
            normed_ref[:, lanes] = (hidden_ref[:, lanes].astype(F32) * scale * fgain_ref[:, lanes]).astype(BF16)

        def expert_step(lanes):
            g = dot(normed_ref[...], wg_ref[0, :, lanes])
            v = dot(normed_ref[...], wu_ref[0, :, lanes])
            inner_ref[:, lanes] = (jax.nn.silu(g) * v).astype(BF16)

        for c in range(5):
            expert_step(slice(c * 256, (c + 1) * 256))
        expert_step(slice(1280, 1408))

        for half in range(2):
            for c in range(4):
                lanes = slice(half * 1024 + c * 256, half * 1024 + (c + 1) * 256)
                y = dot(inner_ref[...], wd_ref[0, :, lanes]).astype(BF16)
                for r in range(2):
                    slots[r, 0:64, c * 256 : (c + 1) * 256] = y[r * 64 : (r + 1) * 64]

            def put_return(at, block):
                ret_out[first + at : first + at + 16, half] = block

            pack(lambda r, at, j: slots[r, at : at + 16, j * 128 : (j + 1) * 128], swap, put_return, 64)
        send_some(first, last, ret_out, ret_in, all_send.at[3 + n], all_recv.at[3 + n], -1)
    ret_in[0] = ret_out[0]

    y = [own_ref[:, c * 256 : (c + 1) * 256].astype(F32) for c in range(8)]
    for n, (first, last) in enumerate(PARTS):
        all_of(max(first, 1), last, ret_out, ret_in, all_send.at[3 + n], all_recv.at[3 + n]).wait_recv()
        for half in range(2):

            def put_back(r, at, j, rows):
                back_ref[r, at : at + 16, j * 128 : (j + 1) * 128] = rows

            unpack(lambda at: ret_in[first + at : first + at + 16, half], swap, put_back, 64)
            for c in range(4):
                lanes = slice(c * 256, (c + 1) * 256)
                for r in range(2):
                    for part in parts[r]:
                        y[4 * half + c] = y[4 * half + c] + dot(part[:, first:last], back_ref[r, :, lanes])
    for c in range(8):
        out_ref[:, c * 256 : (c + 1) * 256] = y[c].astype(BF16)

    all_of(1, 128, res_out, res_in, all_send.at[0], all_recv.at[0]).wait_send()
    for n, (first, last) in enumerate(PARTS):
        first = max(first, 1)
        all_of(first, last, mix_out, mix_in, all_send.at[1 + n], all_recv.at[1 + n]).wait_send()
        all_of(first, last, ret_out, ret_in, all_send.at[3 + n], all_recv.at[3 + n]).wait_send()


def local(
    wide_inputs, narrow_inputs, wide_poles, narrow_poles, step_sizes, forget, wide_in_map,
    narrow_in_map, wide_out_map, narrow_out_map, skip_weight, gate_mix, residual, mixer_gain,
    out_proj, ffn_gain, routes, route_weights, gate_proj, up_proj, down_proj,
):
    ins = (
        wide_inputs, narrow_inputs, wide_poles, narrow_poles, step_sizes, forget.reshape(64, 128),
        wide_in_map.reshape(2, 2, 256, 64), narrow_in_map.reshape(2, 2, 256, 32),
        wide_out_map.reshape(2, 2, 256, 64), narrow_out_map.reshape(2, 2, 256, 32),
        skip_weight, gate_mix.reshape(2, 256, 16), residual, mixer_gain.reshape(1, 1024), out_proj,
        ffn_gain.reshape(1, 2048), routes.T, route_weights.T, gate_proj, up_proj, down_proj,
        jnp.asarray(STEPS, jnp.int32), jnp.asarray(STEPS, jnp.int32).T,
    )
    scratch = [pltpu.VMEM(a.shape, a.dtype) for a in ins]
    scratch += [
        pltpu.VMEM((2, 2, 2, 128, 512), BF16),
        pltpu.VMEM((2, 2, 2, 128, 256), BF16),
        pltpu.VMEM((2, 2, 2, 128, 512), BF16),
        pltpu.VMEM((2, 2, 2, 128, 256), BF16),
        pltpu.VMEM((2, 2, 128, NL), F32),
        pltpu.VMEM((2, 128, NL), F32),
        pltpu.VMEM((2, 192, NL), BF16),
        pltpu.VMEM((2, 2, 8, NL), F32),
        pltpu.VMEM((2, 2, 8, NL), F32),
        pltpu.VMEM((8, NL), F32),
        pltpu.VMEM((3, 16, 448), BF16),
        pltpu.VMEM((3, 4, 16, 448), BF16),
        pltpu.VMEM((2, 64, 512), BF16),
        pltpu.VMEM((64, 512), BF16),
        pltpu.VMEM((128, 2, 16, 128), BF16),
        pltpu.VMEM((128, 2, 16, 128), BF16),
        pltpu.VMEM((128, 16, 128), BF16),
        pltpu.VMEM((128, 16, 128), BF16),
        pltpu.VMEM((128, 2, 16, 128), BF16),
        pltpu.VMEM((128, 2, 16, 128), BF16),
        pltpu.VMEM((2, 128, 1024), BF16),
        pltpu.VMEM((2, 128, 2048), BF16),
        pltpu.VMEM((128, 1024), BF16),
        pltpu.VMEM((128, 2048), BF16),
        pltpu.VMEM((128, 2048), BF16),
        pltpu.VMEM((128, 1408), BF16),
        pltpu.VMEM((2, 64, 1024), BF16),
        pltpu.VMEM((64, 2048), BF16),
        pltpu.SemaphoreType.DMA((23,)),
        pltpu.SemaphoreType.DMA((3, 4)),
        pltpu.SemaphoreType.DMA((3, 4)),
        pltpu.SemaphoreType.DMA,
        pltpu.SemaphoreType.DMA,
        pltpu.SemaphoreType.DMA((7,)),
        pltpu.SemaphoreType.DMA((7,)),
        pltpu.SemaphoreType.REGULAR((3,)),
    ]
    return pl.pallas_call(
        layer_kernel,
        out_shape=jax.ShapeDtypeStruct((64, 2048), BF16),
        in_specs=[pl.BlockSpec(memory_space=pl.ANY)] * 23,
        out_specs=pl.BlockSpec(memory_space=pltpu.VMEM),
        scratch_shapes=scratch,
        compiler_params=pltpu.CompilerParams(
            collective_id=0, has_side_effects=True, vmem_limit_bytes=60 * 1024 * 1024
        ),
        name="layer",
    )(*ins)


def solution(mesh):
    finer = Mesh(mesh.devices.reshape(4, 4, 4, mesh.shape["tp"]), ("sp_0", "sp_1", "sp_2", "tp"))
    return jax.shard_map(
        local,
        mesh=finer,
        in_specs=(
            P(SP, "tp"),
            P(SP, "tp"),
            P(None, None, "tp", None),
            P(None, None, "tp", None),
            P(None, None, "tp"),
            P(None, None, "tp", SP),
            P(None, None, "tp", None, None),
            P(None, None, "tp", None, None),
            P(None, None, "tp", None, None),
            P(None, None, "tp", None, None),
            P(None, "tp"),
            P(None, "tp", None, None),
            P(SP_TP, None),
            P(),
            P(),
            P(),
            P(SP_TP, None),
            P(SP_TP, None),
            P(SP_TP, None, None),
            P(SP_TP, None, None),
            P(SP_TP, None, None),
        ),
        out_specs=P(SP_TP, None),
        check_vma=False,
    )
```

```python
import functools

import jax
import jax.numpy as jnp
from jax import lax
from jax.experimental import pallas as pl
from jax.experimental.pallas import tpu as pltpu
from jax.sharding import Mesh
from jax.sharding import PartitionSpec as P

SP = ("sp_0", "sp_1", "sp_2")
SP_TP = ("sp_0", "sp_1", "sp_2", "tp")
MESH = pl.DeviceIdType.MESH
epsilon = 1e-06
F32 = jnp.float32
BF16 = jnp.bfloat16
NL = 1536
SETS = ((64, 0), (32, 1024))
CHUNK = 512
BATCHES = ((108, 128), (86, 108), (62, 86), (1, 62))
PARTS = ((64, 128), (0, 64))


def dot(a, b):
    return lax.dot_general(a, b, (((1,), (0,)), ((), ())), preferred_element_type=F32)


def dot_nt(a, b):
    return lax.dot_general(a, b, (((1,), (1,)), ((), ())), preferred_element_type=F32)


def split3(x):
    first = x.astype(BF16)
    rest = x - first.astype(F32)
    second = rest.astype(BF16)
    third = (rest - second.astype(F32)).astype(BF16)
    return first, second, third


def iota(shape, dim):
    return lax.broadcasted_iota(jnp.int32, shape, dim)


def cmul(ar, ai, br, bi):
    return ar * br - ai * bi, ar * bi + ai * br


def square(ar, ai):
    return ar * ar - ai * ai, 2.0 * ar * ai


def scattered():
    steps = [(o // 32, o // 8 % 4, o // 2 % 4, o % 2) for o in range(128)]
    return [steps[o] for o in sorted(range(128), key=lambda o: (o > 0, o * 37 % 128))]


STEPS = scattered()
SIZES = (4, 4, 4, 2)


def send_some(first, last, out, arrived, send_sem, recv_sem, way=1):
    there = [
        [lax.rem(lax.axis_index(a) + n + way * s, n) for s in range(n)] for a, n in zip(SP_TP, SIZES)
    ]
    for o in reversed(range(max(first, 1), last)):
        pltpu.make_async_remote_copy(
            src_ref=out.at[o], dst_ref=arrived.at[o], send_sem=send_sem, recv_sem=recv_sem,
            device_id={a: there[k][STEPS[o][k]] for k, a in enumerate(SP_TP)}, device_id_type=MESH,
        ).start()


def all_of(first, last, out, arrived, send_sem, recv_sem):
    return pltpu.make_async_remote_copy(
        src_ref=out.at[pl.ds(first, last - first)], dst_ref=arrived.at[pl.ds(first, last - first)],
        send_sem=send_sem, recv_sem=recv_sem, device_id={"tp": 1 - lax.axis_index("tp")},
        device_id_type=MESH,
    )


def swap_matrix():
    r, c = iota((256, 256), 0), iota((256, 256), 1)
    return (lax.rem(r, 16) * 16 + r // 16 == c).astype(BF16)


def pack(rows, swap, put, blocks):
    for k in range(0, blocks, 32):
        both = jnp.concatenate(
            [
                jnp.concatenate([rows(q // 8, k + 16 * side, q % 8) for q in range(16)], axis=0)
                for side in range(2)
            ],
            axis=1,
        )
        done = dot(swap, both).astype(BF16)
        for side in range(2):
            put(k + 16 * side, done[:, side * 128 : (side + 1) * 128].reshape(16, 16, 128))


def unpack(block, swap, put, blocks):
    for k in range(0, blocks, 32):
        both = jnp.concatenate(
            [block(k + 16 * side).reshape(256, 128) for side in range(2)], axis=1
        )
        done = dot(swap, both).astype(BF16)
        for side in range(2):
            for q in range(16):
                put(q // 8, k + 16 * side, q % 8, done[q * 16 : (q + 1) * 16, side * 128 : (side + 1) * 128])


def layer_kernel(*refs):
    ins, out_ref, held = refs[:23], refs[23], refs[24 : 24 + 23]
    (win_w, win_n, wout_w, wout_n, xs, es, spread, carry_ref, prod_ref, lam_ref, send, recv, mine, theirs,
     res_out, res_in, mix_out, mix_in, ret_out, ret_in, slots, rows_ref, mixed_ref, hidden_ref, normed_ref, inner_ref,
     back_ref, own_ref,
     load_sem, send_sem, recv_sem, tp_send, tp_recv, all_send, all_recv, known_sem) = refs[47:]
    axes = ("sp_2", "sp_1", "sp_0")
    pos = [lax.axis_index(a) for a in axes]
    core = lax.axis_index("tp")

    barrier = pltpu.get_barrier_semaphore()

    def greet(semaphore, axis, place, size):
        for o in range(1, size):
            pl.semaphore_signal(semaphore, inc=1, device_id={axis: lax.rem(place + o, size)}, device_id_type=MESH)

    for a, p in zip(axes, pos):
        greet(barrier, a, p, 4)
    greet(barrier, "tp", core, 2)
    loads = [pltpu.make_async_copy(a, b, load_sem.at[k]) for k, (a, b) in enumerate(zip(ins, held))]
    order = [2, 3, 4, 6, 7, 0, 1, 5, 16, 12, 21, 22, 8, 9, 10, 11, 13, 15, 17, 14, 18, 19, 20]
    for k in order[:19]:
        loads[k].start()
    (uw_ref, un_ref, pw_ref, pn_ref, step_ref, forget_ref, inw_ref, inn_ref, ow_ref, on_ref,
     skip_ref, gate_ref, residual_ref, mgain_ref, outp_ref, fgain_ref, routes_ref, weights_ref,
     wg_ref, wu_ref, wd_ref, down_ref, across_ref) = held
    for k in order[:8]:
        loads[k].wait()

    def spreader(n):
        tiler = (iota((n, 8 * n), 0) == lax.rem(iota((n, 8 * n), 1), n)).astype(BF16)
        return tiler, iota((128, 8 * n), 0) // 16 == iota((128, 8 * n), 1) // n

    def build_out():
        for n, o_ref, wout in ((64, ow_ref, wout_w), (32, on_ref, wout_n)):
            tiler, keep = spreader(n)
            for d in range(2):
                for ri in range(2):
                    for h in range(2):
                        o = o_ref[d, ri, h * 128 : (h + 1) * 128, :]
                        o = (-o if ri else o).astype(BF16)
                        wout[d, ri, h] = jnp.where(keep, dot(o, tiler), 0.0).astype(BF16)

    for s, (p_ref, in_ref, o_ref, win, wout) in enumerate(
        ((pw_ref, inw_ref, ow_ref, win_w, wout_w), (pn_ref, inn_ref, on_ref, win_n, wout_n))
    ):
        n, first = SETS[s]
        tiler, keep = spreader(n)
        for d in range(2):
            pr = p_ref[d, 0]
            pi = p_ref[d, 1]
            grow = jnp.exp(pr)
            lre = grow * jnp.cos(pi)
            lim = grow * jnp.sin(pi)
            nre = lre - 1.0
            step = jnp.sum(jnp.where(iota((16, 16), 0) == iota((16, 16), 1), step_ref[d, s : s + 1, :], 0.0), axis=1, keepdims=True)
            scale = step / (pr * pr + pi * pi)
            fre = (nre * pr + lim * pi) * scale
            fim = (lim * pr - nre * pi) * scale
            for ri, lam in ((0, lre), (1, lim)):
                parts = jnp.concatenate(split3(lam), axis=0)
                for h in range(2):
                    wide = dot(parts, tiler)
                    gr = lax.rem(iota((48, 8 * n), 0), 16)
                    gc = iota((48, 8 * n), 1) // n + 8 * h
                    row = jnp.sum(jnp.where(gr == gc, wide, 0.0), axis=0, keepdims=True)
                    lam_ref[2 * d + ri : 2 * d + ri + 1, first + 8 * n * h : first + 8 * n * (h + 1)] = row
            ere, eim = [], []
            for g in range(16):
                a = in_ref[d, 0, g * 16 : (g + 1) * 16, :]
                b = in_ref[d, 1, g * 16 : (g + 1) * 16, :]
                fr, fi = fre[g : g + 1], fim[g : g + 1]
                ere.append((fr * a - fi * b).astype(BF16))
                eim.append((fr * b + fi * a).astype(BF16))
            for h in range(2):
                for ri, rows in ((0, ere), (1, eim)):
                    part = jnp.concatenate(rows[8 * h : 8 * h + 8], axis=0)
                    win[d, ri, h] = jnp.where(keep, dot(part, tiler), 0.0).astype(BF16)

    for k in order[8:19]:
        loads[k].wait()
    for k in order[19:]:
        loads[k].start()
    pl.semaphore_wait(barrier, 10)
    greet(known_sem.at[0], "sp_2", pos[0], 4)
    pr_ = iota((128, 128), 0)
    pc_ = iota((128, 128), 1)
    perm = (pc_ == lax.rem(pr_, 8) * 16 + pr_ // 8).astype(BF16)
    back = (pr_ == lax.rem(pc_, 8) * 16 + pc_ // 8).astype(BF16)
    u = [dot(perm, uw_ref[...]), dot(perm, un_ref[...])]
    ub = [x.astype(BF16) for x in u]
    for d in range(2):
        for s, win in enumerate((win_w, win_n)):
            n, first = SETS[s]
            for h in range(2):
                at = first + 8 * n * h
                for ri in range(2):
                    xs[d, ri, :, at : at + 8 * n] = dot(ub[s][:, h * 128 : (h + 1) * 128], win[d, ri, h])
    ef = jnp.concatenate(split3(jnp.exp(-forget_ref[...])), axis=0)
    ep = dot_nt(perm, ef).astype(BF16)
    sr = lax.rem(iota((192, NL), 0), 64)
    sc = iota((192, NL), 1)
    group_of = jnp.where(sc < 1024, sc // 64, 16 + (sc - 1024) // 32)
    for d in range(2):
        spread[d] = (sr == group_of + 32 * d).astype(BF16)
        es[d] = dot(ep, spread[d])

    def scan_step(i, state, c, keep_states):
        new = []
        for d in range(2):
            row = i if d == 0 else 15 - i
            at = pl.ds(pl.multiple_of(row * 8, 8), 8)
            lanes = slice(c * CHUNK, (c + 1) * CHUNK)
            lr = lam_ref[2 * d : 2 * d + 1, lanes]
            li = lam_ref[2 * d + 1 : 2 * d + 2, lanes]
            sre, sim = state[3 * d], state[3 * d + 1]
            e = es[d, at, lanes]
            nre = (lr * sre - li * sim) * e + xs[d, 0, at, lanes]
            nim = (lr * sim + li * sre) * e + xs[d, 1, at, lanes]
            if keep_states:
                xs[d, 0, at, lanes] = nre
                xs[d, 1, at, lanes] = nim
            new += [nre, nim, state[3 * d + 2] if keep_states else state[3 * d + 2] * e]
        return tuple(new)

    sub = iota((8, CHUNK), 0)
    ends = [[], []]
    for c in range(NL // CHUNK):
        zero = jnp.zeros((8, CHUNK), F32)
        one = jnp.ones((8, CHUNK), F32)
        state = lax.fori_loop(
            0, 16, lambda i, st: scan_step(i, st, c, False), (zero, zero, one, zero, zero, one)
        )
        lanes = slice(c * CHUNK, (c + 1) * CHUNK)
        for d in range(2):
            sre, sim, g = state[3 * d : 3 * d + 3]
            lr, li = lam_ref[2 * d : 2 * d + 1, lanes], lam_ref[2 * d + 1 : 2 * d + 2, lanes]
            for _ in range(4):
                lr, li = square(lr, li)
            place = sub if d == 0 else 7 - sub
            pre, pim = one, zero
            for k in (1, 2, 4):
                shift = k if d == 0 else 8 - k
                has = place >= k
                before_re = jnp.where(has, pltpu.roll(sre, shift, 0), 0.0) * g
                before_im = jnp.where(has, pltpu.roll(sim, shift, 0), 0.0) * g
                add_re, add_im = cmul(lr, li, before_re, before_im)
                sre, sim = sre + add_re, sim + add_im
                g = g * jnp.where(has, pltpu.roll(g, shift, 0), 1.0)
                tre, tim = cmul(lr, li, pre, pim)
                bit = lax.rem(place // k, 2) == 1
                pre, pim = jnp.where(bit, tre, pre), jnp.where(bit, tim, pim)
                lr, li = square(lr, li)
            edge = 7 if d == 0 else 0
            ends[d].append((sre[edge : edge + 1], sim[edge : edge + 1]))
            shift = 1 if d == 0 else 7
            has = place >= 1
            carry_ref[d, 0, :, lanes] = jnp.where(has, pltpu.roll(sre, shift, 0), 0.0)
            carry_ref[d, 1, :, lanes] = jnp.where(has, pltpu.roll(sim, shift, 0), 0.0)
            gx = jnp.where(has, pltpu.roll(g, shift, 0), 1.0)
            prod_ref[d, 0, :, lanes] = pre * gx
            prod_ref[d, 1, :, lanes] = pim * gx
            lam_ref[4 + 2 * d : 5 + 2 * d, lanes] = lr
            lam_ref[5 + 2 * d : 6 + 2 * d, lanes] = li

    fsum = lax.dot_general(
        jnp.ones((8, 128), F32), forget_ref[...], (((1,), (1,)), ((), ())),
        preferred_element_type=F32, precision=lax.Precision.HIGHEST,
    )[0:1]
    total = [
        [jnp.concatenate([e[q] for e in ends[d]], axis=1) for q in range(2)] for d in range(2)
    ]
    power = [[lam_ref[4 + 2 * d + q : 5 + 2 * d + q, :] for q in range(2)] for d in range(2)]
    enter = None
    carry_copies = []
    pl.semaphore_wait(known_sem.at[0], 3)
    greet(known_sem.at[1], "sp_1", pos[1], 4)
    for stage, a in enumerate(axes):
        p = pos[stage]
        lines = [
            total[d][q][:, 384 * k : 384 * (k + 1)] for d in range(2) for q in range(2) for k in range(4)
        ]
        sums_sent = [x.astype(F32) for x in split3(fsum)] + [jnp.zeros((1, 64), F32)] * 13
        send[stage] = jnp.concatenate(
            [jnp.concatenate(lines, axis=0), jnp.concatenate(sums_sent, axis=0)], axis=1
        ).astype(BF16)
        copies = []
        for o in (1, 3, 2):
            there = lax.rem(p + o, 4)
            copies.append(
                pltpu.make_async_remote_copy(
                    src_ref=send.at[stage],
                    dst_ref=recv.at[stage, p],
                    send_sem=send_sem.at[stage, o],
                    recv_sem=recv_sem.at[stage, p],
                    device_id={a: there},
                    device_id_type=MESH,
                )
            )
            copies[-1].start()
        if stage == 1:
            build_out()
        if stage == 0:
            swap = swap_matrix()
            earlier = (iota((64, 64), 0) < iota((64, 64), 1)).astype(BF16)
            def numbers(steps):
                there = [lax.rem(lax.axis_index(a) + t, n) for a, t, n in zip(SP_TP, steps, SIZES)]
                return ((there[0] * 4 + there[1]) * 4 + there[2]) * 2 + there[3]

            expert = numbers([down_ref[:, k : k + 1] for k in range(4)])
            named = [(expert == routes_ref[k : k + 1, :]).astype(F32) for k in range(2)]
            count = named[0] + named[1]
            rank = dot(count.astype(BF16), earlier)
            pick = [jnp.where(rank == r, count, 0.0).astype(BF16) for r in range(2)]
            for half in range(2):
                for r in range(2):
                    slots[r] = dot(pick[r], residual_ref[:, half * 1024 : (half + 1) * 1024]).astype(BF16)

                def put_residual(at, block):
                    res_out[at : at + 16, half] = block

                pack(lambda r, at, j: slots[r, at : at + 16, j * 128 : (j + 1) * 128], swap, put_residual, 128)
            pl.semaphore_wait(known_sem.at[1], 3)
            greet(known_sem.at[2], "tp", core, 2)
            pl.semaphore_wait(known_sem.at[2], 1)
        send_some(*BATCHES[stage], res_out, res_in, all_send.at[0], all_recv.at[0])
        for o in (1, 3, 2):
            there = lax.rem(p + o, 4)
            pltpu.make_async_remote_copy(
                src_ref=send.at[stage],
                dst_ref=recv.at[stage, there],
                send_sem=send_sem.at[stage, o],
                recv_sem=recv_sem.at[stage, there],
                device_id={a: there},
                device_id_type=MESH,
            ).wait_recv()
        recv[stage, p] = send[stage]
        came = [recv[stage, k].astype(F32) for k in range(4)]
        sums = jnp.concatenate(
            [jnp.sum(x[0:3, 384:448], axis=0, keepdims=True) for x in came], axis=0
        )
        parts = jnp.concatenate(split3(jnp.exp(-sums)), axis=1)
        for d in range(2):
            g = dot(parts, spread[d])
            lr, li = power[d]
            rre = rim = jnp.zeros((1, NL), F32)
            ire = iim = jnp.zeros((1, NL), F32)
            are, aim = jnp.ones((1, NL), F32), jnp.zeros((1, NL), F32)
            jre, jim = are, aim
            for step in range(4):
                k = step if d == 0 else 3 - step
                here = k == p
                ire, iim = jnp.where(here, rre, ire), jnp.where(here, rim, iim)
                nearer = (k < p) if d == 0 else (k > p)
                gr, gi = lr * g[k : k + 1], li * g[k : k + 1]
                tre, tim = (
                    jnp.concatenate([came[k][r : r + 1, 0:384] for r in range(at, at + 4)], axis=1)
                    for at in (8 * d, 8 * d + 4)
                )
                rre, rim = cmul(gr, gi, rre, rim)
                rre, rim = rre + tre, rim + tim
                nre, nim = cmul(gr, gi, jre, jim)
                jre, jim = jnp.where(nearer, nre, jre), jnp.where(nearer, nim, jim)
            total[d] = [rre, rim]
            lr, li = square(*square(lr, li))
            power[d] = [lr, li]
            if enter is None or len(enter) < 2:
                enter = (enter or []) + [[ire, iim, jre, jim]]
            else:
                bre, bim, cre, cim = enter[d]
                add_re, add_im = cmul(cre, cim, ire, iim)
                ncre, ncim = cmul(cre, cim, jre, jim)
                enter[d] = [bre + add_re, bim + add_im, ncre, ncim]
        fsum = jnp.sum(sums, axis=0, keepdims=True)
        carry_copies += copies

    send_some(*BATCHES[3], res_out, res_in, all_send.at[0], all_recv.at[0])
    res_in[0] = res_out[0]
    for c in range(NL // CHUNK):
        lanes = slice(c * CHUNK, (c + 1) * CHUNK)
        state = []
        for d in range(2):
            cre, cim = enter[d][0][:, lanes], enter[d][1][:, lanes]
            add_re, add_im = cmul(prod_ref[d, 0, :, lanes], prod_ref[d, 1, :, lanes], cre, cim)
            state += [carry_ref[d, 0, :, lanes] + add_re, carry_ref[d, 1, :, lanes] + add_im, jnp.zeros((8, 128), F32)]
        lax.fori_loop(0, 16, lambda i, st: scan_step(i, st, c, True), tuple(state))

    for s, wout in enumerate((wout_w, wout_n)):
        n, first = SETS[s]
        for h in range(2):
            at = first + 8 * n * h
            y = None
            for d in range(2):
                for ri in range(2):
                    term = dot_nt(xs[d, ri, :, at : at + 8 * n].astype(BF16), wout[d, ri, h])
                    y = term if y is None else y + term
            ch = slice(h * 128, (h + 1) * 128)
            y = y + skip_ref[s : s + 1, ch].astype(F32) * u[s][:, ch]
            active = jax.nn.gelu(y, approximate=True)
            gr = iota((16, 128), 0)
            gc = iota((16, 128), 1)
            tiler = (gr == lax.rem(gc, 16)).astype(BF16)
            gate = dot(gate_ref[s, ch, :], tiler)
            gate = jnp.where(iota((128, 128), 0) // 16 == iota((128, 128), 1) // 16, gate, 0.0).astype(BF16)
            opened = jax.nn.sigmoid(dot(active.astype(BF16), gate))
            done = dot(back, (active * opened).astype(BF16)).astype(BF16)
            for half in range(2):
                mine[half, :, s * 256 + h * 128 : s * 256 + (h + 1) * 128] = done[half * 64 : (half + 1) * 64]

    copy = pltpu.make_async_remote_copy(
        src_ref=mine.at[1 - core],
        dst_ref=theirs,
        send_sem=tp_send,
        recv_sem=tp_recv,
        device_id={"tp": 1 - core},
        device_id_type=MESH,
    )
    copy.start()
    copy.wait_recv()

    own, other = mine[core].astype(F32), theirs[...].astype(F32)
    low = jnp.where(core == 0, own, other)
    high = jnp.where(core == 0, other, own)
    joined = jnp.concatenate([low[:, :256], high[:, :256], low[:, 256:], high[:, 256:]], axis=1)
    scale = lax.rsqrt(jnp.mean(joined * joined, axis=1, keepdims=True) + epsilon)
    mixed = (joined * scale * mgain_ref[...]).astype(BF16)
    for n, (first, last) in enumerate(PARTS):
        for r in range(2):
            slots[r, 0:64] = dot(pick[r][first:last], mixed).astype(BF16)

        def put_mixed_out(at, block):
            mix_out[first + at : first + at + 16] = block

        pack(lambda r, at, j: slots[r, at : at + 16, j * 128 : (j + 1) * 128], swap, put_mixed_out, 64)
        send_some(first, last, mix_out, mix_in, all_send.at[1 + n], all_recv.at[1 + n])
    mix_in[0] = mix_out[0]

    loads[14].wait()
    for c in range(8):
        lanes = slice(c * 256, (c + 1) * 256)
        own_ref[:, lanes] = (
            residual_ref[:, lanes].astype(F32) + dot(mixed, outp_ref[:, lanes])
        ).astype(BF16)
    all_of(1, 128, res_out, res_in, all_send.at[0], all_recv.at[0]).wait_recv()
    for n, (first, last) in enumerate(PARTS):
        for half in range(2):

            def put_rows(r, at, j, rows):
                lanes = half * 1024 + j * 128
                rows_ref[n, r * 64 + at : r * 64 + at + 16, lanes : lanes + 128] = rows

            unpack(lambda at: res_in[first + at : first + at + 16, half], swap, put_rows, 64)

    eye = iota((64, 64), 0) == iota((64, 64), 1)
    def column(row):
        return jnp.sum(jnp.where(eye, row, 0.0), axis=1, keepdims=True)
    experts = numbers([across_ref[k : k + 1, :] for k in range(4)]).astype(F32)
    hits = [(column(routes_ref[k : k + 1, :].astype(F32)) == experts).astype(F32) for k in range(2)]
    w = [column(weights_ref[k : k + 1, :]) for k in range(2)]
    both = w[0] + w[1]
    before = (iota((64, 64), 1) < iota((64, 64), 0)).astype(BF16)
    ranks = dot(before, (hits[0] + hits[1]).astype(BF16))
    shares = hits[0] * (w[0] / both) + hits[1] * (w[1] / both)
    parts = []
    for r in range(2):
        share = jnp.where(ranks == r, shares, 0.0)
        first = share.astype(BF16)
        parts.append((first, (share - first.astype(F32)).astype(BF16)))

    for k in order[20:]:
        loads[k].wait()
    for n, (first, last) in enumerate(PARTS):
        all_of(max(first, 1), last, mix_out, mix_in, all_send.at[1 + n], all_recv.at[1 + n]).wait_recv()

        def put_mixed(r, at, j, rows):
            mixed_ref[r * 64 + at : r * 64 + at + 16, j * 128 : (j + 1) * 128] = rows

        unpack(lambda at: mix_in[first + at : first + at + 16], swap, put_mixed, 64)
        square_sum = jnp.zeros((128, 1), F32)
        for c in range(8):
            lanes = slice(c * 256, (c + 1) * 256)
            h = (rows_ref[n, :, lanes].astype(F32) + dot(mixed_ref[...], outp_ref[:, lanes])).astype(BF16)
            hidden_ref[:, lanes] = h
            wide = h.astype(F32)
            square_sum = square_sum + jnp.sum(wide * wide, axis=1, keepdims=True)
        scale = lax.rsqrt(square_sum / 2048.0 + epsilon)
        for c in range(8):
            lanes = slice(c * 256, (c + 1) * 256)
            normed_ref[:, lanes] = (hidden_ref[:, lanes].astype(F32) * scale * fgain_ref[:, lanes]).astype(BF16)

        def expert_step(lanes):
            g = dot(normed_ref[...], wg_ref[0, :, lanes])
            v = dot(normed_ref[...], wu_ref[0, :, lanes])
            inner_ref[:, lanes] = (jax.nn.silu(g) * v).astype(BF16)

        for c in range(5):
            expert_step(slice(c * 256, (c + 1) * 256))
        expert_step(slice(1280, 1408))

        for half in range(2):
            for c in range(4):
                lanes = slice(half * 1024 + c * 256, half * 1024 + (c + 1) * 256)
                y = dot(inner_ref[...], wd_ref[0, :, lanes]).astype(BF16)
                for r in range(2):
                    slots[r, 0:64, c * 256 : (c + 1) * 256] = y[r * 64 : (r + 1) * 64]

            def put_return(at, block):
                ret_out[first + at : first + at + 16, half] = block

            pack(lambda r, at, j: slots[r, at : at + 16, j * 128 : (j + 1) * 128], swap, put_return, 64)
        send_some(first, last, ret_out, ret_in, all_send.at[3 + n], all_recv.at[3 + n], -1)
    ret_in[0] = ret_out[0]

    y = [own_ref[:, c * 256 : (c + 1) * 256].astype(F32) for c in range(8)]
    for n, (first, last) in enumerate(PARTS):
        all_of(max(first, 1), last, ret_out, ret_in, all_send.at[3 + n], all_recv.at[3 + n]).wait_recv()
        for half in range(2):

            def put_back(r, at, j, rows):
                back_ref[r, at : at + 16, j * 128 : (j + 1) * 128] = rows

            unpack(lambda at: ret_in[first + at : first + at + 16, half], swap, put_back, 64)
            for c in range(4):
                lanes = slice(c * 256, (c + 1) * 256)
                for r in range(2):
                    for part in parts[r]:
                        y[4 * half + c] = y[4 * half + c] + dot(part[:, first:last], back_ref[r, :, lanes])
    for c in range(8):
        out_ref[:, c * 256 : (c + 1) * 256] = y[c].astype(BF16)

    copy.wait_send()
    for copy in carry_copies:
        copy.wait_send()
    all_of(1, 128, res_out, res_in, all_send.at[0], all_recv.at[0]).wait_send()
    for n, (first, last) in enumerate(PARTS):
        first = max(first, 1)
        all_of(first, last, mix_out, mix_in, all_send.at[1 + n], all_recv.at[1 + n]).wait_send()
        all_of(first, last, ret_out, ret_in, all_send.at[3 + n], all_recv.at[3 + n]).wait_send()


def local(
    wide_inputs, narrow_inputs, wide_poles, narrow_poles, step_sizes, forget, wide_in_map,
    narrow_in_map, wide_out_map, narrow_out_map, skip_weight, gate_mix, residual, mixer_gain,
    out_proj, ffn_gain, routes, route_weights, gate_proj, up_proj, down_proj,
):
    ins = (
        wide_inputs, narrow_inputs, wide_poles, narrow_poles, step_sizes, forget.reshape(64, 128),
        wide_in_map.reshape(2, 2, 256, 64), narrow_in_map.reshape(2, 2, 256, 32),
        wide_out_map.reshape(2, 2, 256, 64), narrow_out_map.reshape(2, 2, 256, 32),
        skip_weight, gate_mix.reshape(2, 256, 16), residual, mixer_gain.reshape(1, 1024), out_proj,
        ffn_gain.reshape(1, 2048), routes.T, route_weights.T, gate_proj, up_proj, down_proj,
        jnp.asarray(STEPS, jnp.int32), jnp.asarray(STEPS, jnp.int32).T,
    )
    scratch = [pltpu.VMEM(a.shape, a.dtype) for a in ins]
    scratch += [
        pltpu.VMEM((2, 2, 2, 128, 512), BF16),
        pltpu.VMEM((2, 2, 2, 128, 256), BF16),
        pltpu.VMEM((2, 2, 2, 128, 512), BF16),
        pltpu.VMEM((2, 2, 2, 128, 256), BF16),
        pltpu.VMEM((2, 2, 128, NL), F32),
        pltpu.VMEM((2, 128, NL), F32),
        pltpu.VMEM((2, 192, NL), BF16),
        pltpu.VMEM((2, 2, 8, NL), F32),
        pltpu.VMEM((2, 2, 8, NL), F32),
        pltpu.VMEM((8, NL), F32),
        pltpu.VMEM((3, 16, 448), BF16),
        pltpu.VMEM((3, 4, 16, 448), BF16),
        pltpu.VMEM((2, 64, 512), BF16),
        pltpu.VMEM((64, 512), BF16),
        pltpu.VMEM((128, 2, 16, 128), BF16),
        pltpu.VMEM((128, 2, 16, 128), BF16),
        pltpu.VMEM((128, 16, 128), BF16),
        pltpu.VMEM((128, 16, 128), BF16),
        pltpu.VMEM((128, 2, 16, 128), BF16),
        pltpu.VMEM((128, 2, 16, 128), BF16),
        pltpu.VMEM((2, 128, 1024), BF16),
        pltpu.VMEM((2, 128, 2048), BF16),
        pltpu.VMEM((128, 1024), BF16),
        pltpu.VMEM((128, 2048), BF16),
        pltpu.VMEM((128, 2048), BF16),
        pltpu.VMEM((128, 1408), BF16),
        pltpu.VMEM((2, 64, 1024), BF16),
        pltpu.VMEM((64, 2048), BF16),
        pltpu.SemaphoreType.DMA((23,)),
        pltpu.SemaphoreType.DMA((3, 4)),
        pltpu.SemaphoreType.DMA((3, 4)),
        pltpu.SemaphoreType.DMA,
        pltpu.SemaphoreType.DMA,
        pltpu.SemaphoreType.DMA((7,)),
        pltpu.SemaphoreType.DMA((7,)),
        pltpu.SemaphoreType.REGULAR((3,)),
    ]
    return pl.pallas_call(
        layer_kernel,
        out_shape=jax.ShapeDtypeStruct((64, 2048), BF16),
        in_specs=[pl.BlockSpec(memory_space=pl.ANY)] * 23,
        out_specs=pl.BlockSpec(memory_space=pltpu.VMEM),
        scratch_shapes=scratch,
        compiler_params=pltpu.CompilerParams(
            collective_id=0, has_side_effects=True, vmem_limit_bytes=60 * 1024 * 1024
        ),
        name="layer",
    )(*ins)


def solution(mesh):
    finer = Mesh(mesh.devices.reshape(4, 4, 4, mesh.shape["tp"]), ("sp_0", "sp_1", "sp_2", "tp"))
    return jax.shard_map(
        local,
        mesh=finer,
        in_specs=(
            P(SP, "tp"),
            P(SP, "tp"),
            P(None, None, "tp", None),
            P(None, None, "tp", None),
            P(None, None, "tp"),
            P(None, None, "tp", SP),
            P(None, None, "tp", None, None),
            P(None, None, "tp", None, None),
            P(None, None, "tp", None, None),
            P(None, None, "tp", None, None),
            P(None, "tp"),
            P(None, "tp", None, None),
            P(SP_TP, None),
            P(),
            P(),
            P(),
            P(SP_TP, None),
            P(SP_TP, None),
            P(SP_TP, None, None),
            P(SP_TP, None, None),
            P(SP_TP, None, None),
        ),
        out_specs=P(SP_TP, None),
        check_vma=False,
    )
```
